32 devices in a mesh: kv: 16 (over z, y, x), tp: 2 (over core).
Axes of the slice: x: 2, y: 2, z: 4, core: 2. Of those that a mesh axis runs over, the one named last changes fastest.
Arguments:
- tokens: bfloat16 [64, 4096], P(None, 'kv')
- lengths: int32 [16], replicated, may hold values from 1 to 4, 28 in all
- memory: float32 [16, 16, 128, 128], P('kv', 'tp'), may hold values from -0.6 to 0.6
- norm_gain: float32 [4096], P('kv'), may hold values from 0.1 to 1.9
- w_query: bfloat16 [4096, 2048], P('kv', 'tp'), may hold values from -0.09375 to 0.09375
- w_key: bfloat16 [4096, 2048], P('kv', 'tp'), may hold values from -0.09375 to 0.09375
- w_value: bfloat16 [4096, 2048], P('kv', 'tp'), may hold values from -0.09375 to 0.09375
- w_outgate: bfloat16 [4096, 2048], P('kv', 'tp'), may hold values from -0.09375 to 0.09375
- w_alpha: bfloat16 [4096, 16], P('kv'), may hold values from -0.09375 to 0.09375
- w_beta: bfloat16 [4096, 16], P('kv'), may hold values from -0.09375 to 0.09375
- decay_log: float32 [16], P('tp'), may hold values from -4 to 0.5
- decay_bias: float32 [16], P('tp'), may hold values from -1 to 1
- head_gain: float32 [128], replicated, may hold values from 0.1 to 1.9
- w_output: bfloat16 [2048, 4096], P('tp', 'kv'), may hold values from -0.125 to 0.125
- mlp_gain: float32 [4096], P('kv'), may hold values from 0.1 to 1.9
- w_gate: bfloat16 [4096, 11264], P('kv', 'tp'), may hold values from -0.09375 to 0.09375
- w_up: bfloat16 [4096, 11264], P('kv', 'tp'), may hold values from -0.09375 to 0.09375
- w_down: bfloat16 [11264, 4096], P('tp', 'kv'), may hold values from -0.0546875 to 0.0546875
Outputs:
- layer_out: bfloat16 [64, 4096], P(None, 'kv')
- new_memory: float32 [16, 16, 128, 128], P('kv', 'tp')
The draws below stay inside these ranges and needn't reach their ends.
Inputs may be any that keep to these rules, and one draw needn't show every extreme that they name: How many of a sequence's 4 slots hold live tokens; the live ones come first; the lengths add up to seven quarters of 16, rounded down.
All inputs are finite; a program needn't handle non-finite values.
Results may differ from the reference program's by a relative error of at most 0.012.
Values may be sent and summed in bfloat16 or wider, within the bound.
A program may use at most 64 MiB of HBM per device.

```python
import math
import jax
import jax.numpy as jnp
import numpy as np
from jax import lax

D = 4096
H = 16
DK = 128
DV = 128
FF = 11264
NEW = 4
SEQS = 16


def draw_tokens(key, part):
    first, second, third = jax.random.split(key, 3)
    total_rows = SEQS * NEW
    column_ramp = jnp.exp(jnp.linspace(math.log(0.5), math.log(2.0), D))
    column_noise = jnp.exp(jax.random.uniform(second, (D,), jnp.float32, math.log(0.7), math.log(1.4)))
    row_scale = jnp.exp(jax.random.uniform(third, (total_rows, 1), jnp.float32, math.log(0.3), math.log(3.0)))
    base = jax.random.normal(first, (total_rows, D), jnp.float32)
    return (base * column_ramp * column_noise * row_scale).astype(jnp.bfloat16)


def level_of(key, extent, pieces, least, largest):
    level = 1.0
    for position, parts in pieces:
        draws = jax.random.uniform(jax.random.fold_in(jax.random.fold_in(key, 6), position), (parts,), jnp.float32, least / len(pieces), largest / len(pieces))
        level = level * jnp.repeat(jnp.exp(draws), extent[position] // parts).reshape((-1,) + (1,) * (len(extent) - 1 - position))
    return level


def length_profile(count, total, reach, slope):
    weights = [(1 << 20) // math.isqrt(rank ** slope) + 1 for rank in range(2, count + 1)]
    surplus, counts = total - reach - (count - 1), [1] * (count - 1)
    while surplus > 0:
        movable = [i for i in range(count - 1) if counts[i] < reach]
        whole, budget = sum([weights[i] for i in movable]), surplus
        for i in movable:
            more = min(reach - counts[i], max(1, budget * weights[i] // whole), surplus)
            counts[i] = counts[i] + more
            surplus = surplus - more
    return np.array([reach] + counts)


def ragged(stream_key, count, total, bound, slope):
    if count == 2:
        one = jax.random.randint(stream_key, (), max(1, total - bound), min(bound, total - 1) + 1)
        return jnp.stack([one, total - one])
    sizes = jnp.asarray(length_profile(count, total, bound, slope), jnp.int32)
    pairs = (count - 1) // 2
    giver, sink = sizes[1:1 + 2 * pairs:2], sizes[2:2 + 2 * pairs:2]
    room = jnp.minimum(giver - 1, bound - sink)
    passed = jax.random.randint(jax.random.fold_in(stream_key, 1), (pairs,), 0, 1 << 20) % (room + 1)
    sizes = sizes.at[1:1 + 2 * pairs:2].set(giver - passed).at[2:2 + 2 * pairs:2].set(sink + passed)
    return sizes[jax.random.permutation(jax.random.fold_in(stream_key, 2), count)]


def centred(rng, extent, spread, bound, cuts=(), held_as=jnp.bfloat16):
    gain = level_of(rng, extent, cuts, -0.22, 0.18) if cuts else 1.0
    values = jax.random.normal(rng, extent, jnp.float32) * spread * gain
    return jnp.minimum(jnp.maximum(values, -bound), bound).astype(held_as)


def setup_inputs(seed: int = 0) -> dict:
    streams_of = jax.random.split(jax.random.key(seed), 19)
    return {
        "tokens": draw_tokens(jax.random.fold_in(streams_of[18], 71), 0),
        "lengths": ragged(streams_of[1], SEQS, SEQS * 7 // 4, NEW, 2).astype(jnp.int32),
        "memory": centred(streams_of[2], (SEQS, H, DK, DV), 0.1, 0.6, ((0, 16), (1, 2)), jnp.float32),
        "norm_gain": jnp.clip(1.0 + 0.18 * jax.random.normal(streams_of[3], (D,), jnp.float32), 0.1, 1.9),
        "w_query": centred(streams_of[4], (D, H * DK), D ** -0.5, 0.09375, ((0, 16), (1, 2))),
        "w_key": centred(streams_of[5], (D, H * DK), D ** -0.5, 0.09375, ((0, 16), (1, 2))),
        "w_value": centred(streams_of[6], (D, H * DV), D ** -0.5, 0.09375, ((0, 16), (1, 2))),
        "w_outgate": centred(streams_of[7], (D, H * DV), D ** -0.5, 0.09375, ((0, 16), (1, 2))),
        "w_alpha": centred(streams_of[8], (D, H), D ** -0.5, 0.09375, ((0, 16),)),
        "w_beta": centred(streams_of[9], (D, H), D ** -0.5, 0.09375, ((0, 16),)),
        "decay_log": jnp.clip(-4.0 + 4.5 * jax.random.uniform(streams_of[10], (H,), jnp.float32) ** level_of(streams_of[10], (H,), ((0, 2),), -0.2, 0.2), -4.0, 0.5),
        "decay_bias": jnp.clip(jax.random.uniform(streams_of[11], (H,), jnp.float32, -1.0, 1.0) * level_of(streams_of[11], (H,), ((0, 2),), -0.4, 0.0), -1.0, 1.0),
        "head_gain": jnp.clip(1.0 + 0.18 * jax.random.normal(streams_of[12], (DV,), jnp.float32), 0.1, 1.9),
        "w_output": centred(streams_of[13], (H * DV, D), (H * DV) ** -0.5, 0.125, ((0, 2), (1, 16))),
        "mlp_gain": jnp.clip(1.0 + 0.18 * jax.random.normal(streams_of[14], (D,), jnp.float32), 0.1, 1.9),
        "w_gate": centred(streams_of[15], (D, FF), D ** -0.5, 0.09375, ((0, 16), (1, 2))),
        "w_up": centred(streams_of[16], (D, FF), D ** -0.5, 0.09375, ((0, 16), (1, 2))),
        "w_down": centred(streams_of[17], (FF, D), FF ** -0.5, 0.0546875, ((0, 2), (1, 16))),
    }


epsilon = 1e-06

def unit_rows(values):
    return values * lax.rsqrt(lax.optimization_barrier(jnp.sum(values * values, axis=-1, keepdims=True)) + epsilon)

def advance(memory, queries, key_rows, value_rows, decays, betas):
    outputs = []
    for step in range(queries.shape[1]):
        memory = jnp.exp(decays[:, step])[:, :, None, None] * memory
        predicted = jnp.einsum('shde,shd->she', memory, key_rows[:, step], precision=lax.Precision.HIGHEST)
        correction = betas[:, step][:, :, None] * (value_rows[:, step] - predicted)
        memory = memory + key_rows[:, step][:, :, :, None] * correction[:, :, None, :]
        outputs.append(jnp.einsum('shde,shd->she', memory, queries[:, step], precision=lax.Precision.HIGHEST))
    return (memory, jnp.stack(outputs, axis=1))

def reference(tokens, lengths, memory, norm_gain, w_query, w_key, w_value, w_outgate, w_alpha, w_beta, decay_log, decay_bias, head_gain, w_output, mlp_gain, w_gate, w_up, w_down):
    total_rows = tokens.shape[0]
    token_f = tokens.astype(jnp.float32)
    rstd = lax.rsqrt(lax.optimization_barrier(jnp.mean(token_f * token_f, axis=1, keepdims=True)) + epsilon)
    scaled = (token_f * norm_gain).astype(jnp.bfloat16)

    def project(weight):
        return jnp.dot(scaled, weight, preferred_element_type=jnp.float32) * rstd
    queries = project(w_query).astype(jnp.bfloat16)
    key_rows = project(w_key).astype(jnp.bfloat16)
    value_rows = project(w_value).astype(jnp.bfloat16)
    outgate = project(w_outgate).astype(jnp.bfloat16)
    alphas = project(w_alpha)
    beta_pre = project(w_beta)
    live = jnp.arange(NEW, dtype=jnp.int32)[None, :] < lengths[:, None]
    query_h = unit_rows(queries.astype(jnp.float32).reshape(SEQS, NEW, H, DK)) * DK ** (-0.5)
    key_h = unit_rows(key_rows.astype(jnp.float32).reshape(SEQS, NEW, H, DK))
    value_h = value_rows.astype(jnp.float32).reshape(SEQS, NEW, H, DV)
    decays = -jnp.exp(decay_log) * jax.nn.softplus(alphas + decay_bias)
    decays = jnp.where(live[:, :, None], decays.reshape(SEQS, NEW, H), 0.0)
    betas = jnp.where(live[:, :, None], jax.nn.sigmoid(beta_pre).reshape(SEQS, NEW, H), 0.0)
    new_memory, attended = advance(memory, query_h, key_h, value_h, decays, betas)
    attended = attended * lax.rsqrt(lax.optimization_barrier(jnp.mean(attended * attended, axis=-1, keepdims=True)) + epsilon)
    gate_h = outgate.astype(jnp.float32).reshape(SEQS, NEW, H, DV)
    mixed = (attended * head_gain * jax.nn.silu(gate_h)).astype(jnp.bfloat16).reshape(total_rows, H * DV)
    hidden = (token_f + jnp.dot(mixed, w_output, preferred_element_type=jnp.float32)).astype(jnp.bfloat16)
    hidden_f = hidden.astype(jnp.float32)
    rstd2 = lax.rsqrt(lax.optimization_barrier(jnp.mean(hidden_f * hidden_f, axis=1, keepdims=True)) + epsilon)
    hscaled = (hidden_f * mlp_gain).astype(jnp.bfloat16)
    gate_rows = jnp.dot(hscaled, w_gate, preferred_element_type=jnp.float32) * rstd2
    up_rows = jnp.dot(hscaled, w_up, preferred_element_type=jnp.float32) * rstd2
    active = (jax.nn.silu(gate_rows) * up_rows).astype(jnp.bfloat16)
    result = hidden_f + jnp.dot(active, w_down, preferred_element_type=jnp.float32)
    layer_out = jnp.where(live.reshape(total_rows)[:, None], result, 0.0).astype(jnp.bfloat16)
    return (layer_out, new_memory)
```

```python
import jax
import jax.numpy as jnp
from jax import lax
from jax.experimental import pallas as pl
from jax.experimental.pallas import tpu as pltpu
from jax.sharding import PartitionSpec as P

D = 4096
DK = 128
DV = 128
NEW = 4


epsilon = 1e-06


def unit_rows(values):
    return values * lax.rsqrt(jnp.sum(values * values, axis=-1, keepdims=True) + epsilon)


def advance(memory, queries, key_rows, value_rows, decays, betas):
    outputs = []
    for step in range(queries.shape[1]):
        memory = jnp.exp(decays[:, step])[:, :, None, None] * memory
        predicted = jnp.einsum(
            "shde,shd->she", memory, key_rows[:, step], precision=lax.Precision.HIGHEST
        )
        correction = betas[:, step][:, :, None] * (value_rows[:, step] - predicted)
        memory = memory + key_rows[:, step][:, :, :, None] * correction[:, :, None, :]
        outputs.append(
            jnp.einsum("shde,shd->she", memory, queries[:, step], precision=lax.Precision.HIGHEST)
        )
    return (memory, jnp.stack(outputs, axis=1))


def per_device(
    tokens,
    lengths,
    memory,
    norm_gain,
    w_query,
    w_key,
    w_value,
    w_outgate,
    w_alpha,
    w_beta,
    decay_log,
    decay_bias,
    head_gain,
    w_output,
    mlp_gain,
    w_gate,
    w_up,
    w_down,
):
    total_rows = tokens.shape[0]
    kv_count = lax.axis_size("kv")
    kv_place = lax.axis_index("kv")
    tp_place = lax.axis_index("tp")
    own_rows = total_rows // kv_count
    seq_dev = memory.shape[0]
    heads_dev = memory.shape[1]
    token_f = tokens.astype(jnp.float32)
    squares = jnp.sum(token_f * token_f, axis=1)
    scaled = (token_f * norm_gain).astype(jnp.bfloat16)
    part_query = jnp.dot(scaled, w_query, preferred_element_type=jnp.float32)
    part_key = jnp.dot(scaled, w_key, preferred_element_type=jnp.float32)
    part_value = jnp.dot(scaled, w_value, preferred_element_type=jnp.float32)
    part_gate = jnp.dot(scaled, w_outgate, preferred_element_type=jnp.float32)
    part_alpha = jnp.dot(scaled, w_alpha, preferred_element_type=jnp.float32)
    part_beta = jnp.dot(scaled, w_beta, preferred_element_type=jnp.float32)
    all_squares = lax.psum(squares, "kv")
    sum_query, sum_key, sum_value, sum_gate, sum_alpha, sum_beta = (
        lax.psum_scatter(part_query, "kv", scatter_dimension=0, tiled=True),
        lax.psum_scatter(part_key, "kv", scatter_dimension=0, tiled=True),
        lax.psum_scatter(part_value, "kv", scatter_dimension=0, tiled=True),
        lax.psum_scatter(part_gate, "kv", scatter_dimension=0, tiled=True),
        lax.psum_scatter(part_alpha, "kv", scatter_dimension=0, tiled=True),
        lax.psum_scatter(part_beta, "kv", scatter_dimension=0, tiled=True),
    )
    own_squares = lax.dynamic_slice_in_dim(all_squares, kv_place * own_rows, own_rows)
    rstd = lax.rsqrt(own_squares / D + epsilon)[:, None]
    queries = (sum_query * rstd).astype(jnp.bfloat16)
    key_rows = (sum_key * rstd).astype(jnp.bfloat16)
    value_rows = (sum_value * rstd).astype(jnp.bfloat16)
    outgate = (sum_gate * rstd).astype(jnp.bfloat16)
    alphas = lax.dynamic_slice_in_dim(sum_alpha * rstd, tp_place * heads_dev, heads_dev, 1)
    beta_pre = lax.dynamic_slice_in_dim(sum_beta * rstd, tp_place * heads_dev, heads_dev, 1)
    own_lengths = lax.dynamic_slice_in_dim(lengths, kv_place * seq_dev, seq_dev)
    live = jnp.arange(NEW, dtype=jnp.int32)[None, :] < own_lengths[:, None]
    query_h = unit_rows(queries.astype(jnp.float32).reshape(seq_dev, NEW, heads_dev, DK)) * DK ** (
        -0.5
    )
    key_h = unit_rows(key_rows.astype(jnp.float32).reshape(seq_dev, NEW, heads_dev, DK))
    value_h = value_rows.astype(jnp.float32).reshape(seq_dev, NEW, heads_dev, DV)
    decays = -jnp.exp(decay_log) * jax.nn.softplus(alphas + decay_bias)
    decays = jnp.where(live[:, :, None], decays.reshape(seq_dev, NEW, heads_dev), 0.0)
    betas = jnp.where(
        live[:, :, None], jax.nn.sigmoid(beta_pre).reshape(seq_dev, NEW, heads_dev), 0.0
    )
    new_memory, attended = advance(memory, query_h, key_h, value_h, decays, betas)
    attended = attended * lax.rsqrt(jnp.mean(attended * attended, axis=-1, keepdims=True) + epsilon)
    gate_h = outgate.astype(jnp.float32).reshape(seq_dev, NEW, heads_dev, DV)
    mixed = (
        (attended * head_gain * jax.nn.silu(gate_h))
        .astype(jnp.bfloat16)
        .reshape(own_rows, heads_dev * DV)
    )
    attn_terms = jnp.dot(
        lax.all_gather(mixed, "kv", axis=0, tiled=True),
        w_output,
        preferred_element_type=jnp.float32,
    )
    attn_total = lax.psum(attn_terms, "tp")
    hidden = (token_f + attn_total).astype(jnp.bfloat16)
    hidden_f = hidden.astype(jnp.float32)
    hidden_squares = jnp.sum(hidden_f * hidden_f, axis=1)
    hscaled = (hidden_f * mlp_gain).astype(jnp.bfloat16)
    all_live = (jnp.arange(NEW, dtype=jnp.int32)[None, :] < lengths[:, None]).reshape(total_rows)
    part_gate_rows = jnp.dot(hscaled, w_gate, preferred_element_type=jnp.float32)
    part_up_rows = jnp.dot(hscaled, w_up, preferred_element_type=jnp.float32)
    gate_rows, up_rows, mlp_squares = lax.psum((part_gate_rows, part_up_rows, hidden_squares), "kv")
    rstd2 = lax.rsqrt(mlp_squares / D + epsilon)[:, None]
    active = (jax.nn.silu(gate_rows * rstd2) * (up_rows * rstd2)).astype(jnp.bfloat16)
    feed_terms = jnp.dot(active, w_down, preferred_element_type=jnp.float32)
    feed_total = lax.psum(feed_terms.astype(jnp.bfloat16), "tp").astype(jnp.float32)
    layer_out = jnp.where(all_live[:, None], hidden_f + feed_total, 0.0).astype(jnp.bfloat16)
    return (layer_out, new_memory)


F32 = jnp.float32
BF16 = jnp.bfloat16
HIGH = lax.Precision.HIGHEST
TILE = 128
GROUP = 8


def iota(shape, axis):
    return lax.broadcasted_iota(jnp.int32, shape, axis)


def dot(a, b, precision=None):
    return jnp.dot(a, b, preferred_element_type=F32, precision=precision)


def fused(
    lens_far,
    tokens_far,
    norm_far,
    decay_log_far,
    decay_bias_far,
    head_far,
    mlp_far,
    alpha_far,
    beta_far,
    memory,
    w_query,
    w_key,
    w_value,
    w_outgate,
    w_output,
    w_gate,
    w_up,
    w_down,
    out,
    v_mem,
    lens,
    tokens,
    norm_gain,
    decay_in,
    head_gain,
    mlp_gain,
    v_ab,
    v_proj,
    v_output,
    v_gu,
    v_down,
    proj_send,
    proj_recv,
    proj_part,
    proj_last,
    small_send,
    small_recv,
    small_part,
    small_last,
    rs_buf,
    xs_buf,
    kq_buf,
    r_buf,
    u_buf,
    a_buf,
    mix_buf,
    mix_all,
    tp_send,
    tp_recv,
    sq_send,
    sq_recv,
    gu_send,
    gu_recv,
    gu_part,
    gu_last,
    act_all,
    load_sem,
    send_sem,
    recv_sem,
    tp_sem,
):
    kv_count = mix_all.shape[0]
    me = lax.axis_index("kv")
    tp = lax.axis_index("tp")
    rows, width = tokens.shape
    heads = v_mem.shape[0]
    wide = heads * DV
    compact = tp_send.shape[1]
    groups = compact // GROUP
    zones = kv_count // groups
    chunk = gu_send.shape[2]
    total_width = width * kv_count
    all_heads = v_ab.shape[1]
    zone_me = me // groups
    group_me = lax.rem(me, groups)
    steps = [*range(1, zones), 0]
    side, odd = zone_me // 2, lax.rem(zone_me, 2)

    def zone_of(step):
        if zones != 4:
            return lax.rem(zone_me + step, zones)
        across = (1 - side) * 2
        return [zone_me, across + 1 - odd, across + odd, side * 2 + 1 - odd][step]

    def peer(g):
        return lax.rem(group_me + g, groups)

    barrier = pltpu.get_barrier_semaphore()

    def greet(**where):
        pl.semaphore_signal(
            barrier, inc=1, device_id=where, device_id_type=pl.DeviceIdType.MESH
        )

    for g in range(1, groups):
        greet(kv=zone_me * groups + peer(g))
    for step in steps[:-1]:
        greet(kv=zone_of(step) * groups + group_me)
    greet(tp=1 - tp)

    def load(src, dst, sem):
        return pltpu.make_async_copy(src, dst, load_sem.at[sem])

    half = wide // 2
    halves = [slice(c * half, (c + 1) * half) for c in range(2)]
    load(tokens_far, tokens, 0).start()
    load(norm_far, norm_gain, 1).start()
    load(alpha_far, v_ab.at[0], 2).start()
    load(beta_far, v_ab.at[1], 2).start()
    for c in range(2):
        for p, weight in enumerate((w_query, w_key, w_value, w_outgate)):
            load(weight.at[:, halves[c]], v_proj.at[p, :, halves[c]], 3 + c).start()
    load(lens_far, lens, 5).start()
    load(decay_log_far, decay_in.at[0], 6).start()
    load(decay_bias_far, decay_in.at[1], 6).start()
    load(head_far, head_gain, 7).start()
    load(mlp_far, mlp_gain, 8).start()

    def loaded(ref, sem):
        load(ref, ref, sem).wait()

    plane_sem, gu_sem, near_sem, far_sem = 0, zones, 2 * zones, 3 * zones
    proj_sem, mlp_sem, mix_sem, small_sem, few_sem, sq_sem = range(4 * zones, 4 * zones + 6)

    def remote(src, dst, sent, arrival, partner):
        return pltpu.make_async_remote_copy(
            src_ref=src,
            dst_ref=dst,
            send_sem=send_sem.at[sent],
            recv_sem=recv_sem.at[arrival],
            device_id={"kv": partner},
            device_id_type=pl.DeviceIdType.MESH,
        )

    def arrived(ref, arrival):
        remote(ref, ref, 0, arrival, me).wait_recv()

    def left(ref, sent):
        remote(ref, ref, sent, 0, me).wait_send()

    def tp_swap(phase, value, meanwhile=None):
        tp_send[phase] = value
        swap = pltpu.make_async_remote_copy(
            src_ref=tp_send.at[phase],
            dst_ref=tp_recv.at[phase],
            send_sem=tp_sem.at[phase, 0],
            recv_sem=tp_sem.at[phase, 1],
            device_id={"tp": 1 - tp},
            device_id_type=pl.DeviceIdType.MESH,
        )
        swap.start()
        if meanwhile is not None:
            meanwhile()
        swap.wait()
        return value + tp_recv[phase]

    packed_rows = kv_count * 2 * NEW
    row = iota((packed_rows, rows), 0)
    spread = jnp.where(
        iota((packed_rows, rows), 1) == (row >> 3) * NEW + (row & 3), 1.0, 0.0
    ).astype(BF16)
    seq_row = iota((kv_count, rows), 0)
    seq_row = lax.rem(seq_row, zones) * groups + seq_row // zones
    lane = iota((kv_count, TILE), 1)
    place = iota((TILE, all_heads), 0) & (2 * all_heads - 1)
    head_of = iota((TILE, all_heads), 1)
    one_alpha = jnp.where(place == head_of, 1.0, 0.0).astype(BF16)
    one_beta = jnp.where(place == head_of + all_heads, 1.0, 0.0).astype(BF16)
    loaded(tokens, 0)
    loaded(norm_gain, 1)
    tok = tokens[...]
    scaled = (tok.astype(F32) * norm_gain[...]).astype(BF16)
    wide_scaled = dot(spread, scaled)
    part_of = iota((packed_rows, width), 0) & 7
    low = jnp.where(part_of < NEW, wide_scaled, 0.0).astype(BF16)
    high = jnp.where(part_of >= NEW, wide_scaled, 0.0).astype(BF16)
    loaded(v_ab, 2)
    w_small = (dot(one_alpha, v_ab[0]) + dot(one_beta, v_ab[1])).astype(BF16)
    small = jnp.zeros((kv_count, TILE), F32)
    squares = jnp.zeros((kv_count, TILE), F32)
    for t in range(NEW):
        take = jnp.where(iota((kv_count, rows), 1) == seq_row * NEW + t, 1.0, 0.0).astype(BF16)
        took = lax.dot_general(
            dot(take, scaled).astype(BF16),
            w_small,
            (((1,), (1,)), ((), ())),
            preferred_element_type=F32,
        )
        small = jnp.where(lane // (2 * all_heads) == t, took, small)
        tok_t = dot(take, tok)
        squares = jnp.where(
            lane == t, jnp.sum(tok_t * tok_t, axis=1, keepdims=True), squares
        )
    small_send[:, :, 0, :] = small.reshape(groups, zones, TILE)
    small_send[:, :, 1, :] = squares.reshape(groups, zones, TILE)
    for c in range(2):
        loaded(v_proj.at[:, :, halves[c]], 3 + c)
        parts = [
            dot(low, v_proj[p, :, halves[c]]) + dot(high, v_proj[p + 1, :, halves[c]])
            for p in (0, 2)
        ]
        parts = [part.reshape(kv_count, 2 * NEW, half) for part in parts]
        proj_send[:, :, halves[c]] = jnp.concatenate(parts, axis=1).astype(BF16)
    load(memory, v_mem, 9).start()
    load(w_output, v_output, 10).start()
    load(w_gate, v_gu.at[0], 11).start()
    load(w_up, v_gu.at[1], 11).start()
    load(w_down, v_down, 12).start()

    pl.semaphore_wait(barrier, groups + zones - 1)

    for g in range(1, groups):
        remote(
            small_send.at[peer(g)],
            small_recv.at[group_me],
            0,
            small_sem,
            zone_me * groups + peer(g),
        ).start()

    def send_plane(send, recv, sent, sem, zone):
        for g in range(1, groups):
            remote(
                send.at[zone * groups + peer(g)],
                recv.at[zone * groups + group_me],
                sent,
                sem + zone,
                zone_me * groups + peer(g),
            ).start()

    def sum_plane(send, recv, sem, zone):
        arrived(recv.at[pl.ds(zone * groups, groups - 1)], sem + zone)
        added = send[zone * groups + group_me].astype(F32)
        for g in range(1, groups):
            added = added + recv[zone * groups + peer(g)].astype(F32)
        return added

    def reduce_start(send, recv, part, last, sem, sent, arrival):
        for step in steps[:-1]:
            zone = zone_of(step)
            part[zone] = sum_plane(send, recv, sem, zone).astype(BF16)
            remote(
                part.at[zone], last.at[zone_me], sent, arrival, zone * groups + group_me
            ).start()
        return sum_plane(send, recv, sem, zone_me)

    def reduce_end(added, last, arrival):
        arrived(last.at[pl.ds(0, zones - 1)], arrival)
        for step in steps[:-1]:
            added = added + last[zone_of(step)].astype(F32)
        return added

    for step in steps:
        send_plane(proj_send, proj_recv, 1, plane_sem, zone_of(step))

    loaded(lens, 5)
    loaded(decay_in, 6)
    loaded(head_gain, 7)
    loaded(mlp_gain, 8)
    slots_wide = kv_count * heads * NEW
    shape_a = (1, rows)
    shape_b = (1, slots_wide)
    shape_c = (rows, compact)
    length_a = jnp.zeros(shape_a, jnp.int32)
    start_a = jnp.zeros(shape_a, jnp.int32)
    length_b = jnp.zeros(shape_b, jnp.int32)
    start_b = jnp.zeros(shape_b, jnp.int32)
    length_c = jnp.zeros(shape_c, jnp.int32)
    start_c = jnp.zeros(shape_c, jnp.int32)
    seq_a = iota(shape_a, 1) >> 2
    seq_b = iota(shape_b, 1) >> 5
    seq_c = iota(shape_c, 0) >> 2
    begin = jnp.int32(0)
    for s in range(kv_count):
        length_a = jnp.where(seq_a == s, lens[s], length_a)
        start_a = jnp.where(seq_a == s, begin, start_a)
        length_b = jnp.where(seq_b == s, lens[s], length_b)
        start_b = jnp.where(seq_b == s, begin, start_b)
        length_c = jnp.where(seq_c == s, lens[s], length_c)
        start_c = jnp.where(seq_c == s, begin, start_c)
        begin = begin + lens[s]
    slot_a = iota(shape_a, 1) & 3
    rank_a = jnp.where(slot_a < length_a, start_a + slot_a, -1)
    pack = jnp.where(rank_a == iota((compact, rows), 0), 1.0, 0.0).astype(BF16)
    slot_c = iota(shape_c, 0) & 3
    rank_c = jnp.where(slot_c < length_c, start_c + slot_c, -1)
    unpack = jnp.where(rank_c == iota(shape_c, 1), 1.0, 0.0).astype(BF16)
    slot_b = iota(shape_b, 1) & 3
    head_b = (iota(shape_b, 1) >> 2) & (heads - 1)
    rank_b = jnp.where(slot_b < length_b, head_b * compact + start_b + slot_b, -1)
    collect = jnp.where(rank_b == iota((heads * compact, slots_wide), 0), 1.0, 0.0).astype(BF16)
    tok_packed = dot(pack, tok)

    arrived(small_recv.at[pl.ds(0, groups - 1)], small_sem)
    small = small_send[group_me]
    for g in range(1, groups):
        small = small + small_recv[peer(g)]
    small_part[...] = small
    for step in steps[:-1]:
        zone = zone_of(step)
        remote(
            small_part.at[zone], small_last.at[zone_me], 2, few_sem, zone * groups + group_me
        ).start()

    total = reduce_start(proj_send, proj_recv, proj_part, proj_last, plane_sem, 3, proj_sem)
    arrived(small_last.at[pl.ds(0, zones - 1)], few_sem)
    small = small_part[zone_me]
    for step in steps[:-1]:
        small = small + small_last[zone_of(step)]
    diagonal = iota((NEW, TILE), 0) == iota((NEW, TILE), 1)
    mean_sq = jnp.sum(jnp.where(diagonal, small[1:2, :], 0.0), axis=1, keepdims=True)
    rstd = lax.rsqrt(mean_sq / total_width + epsilon)
    rstd_wide = jnp.broadcast_to(rstd, (NEW, TILE))
    for p in range(4):
        rs_buf[p * NEW : (p + 1) * NEW, :] = rstd_wide
    eye = iota((heads, heads), 0) == iota((heads, heads), 1)
    rate = jnp.sum(jnp.where(eye, jnp.exp(decay_in[0]), 0.0), axis=1, keepdims=True)
    bias = jnp.sum(jnp.where(eye, decay_in[1], 0.0), axis=1, keepdims=True)
    pick = iota((heads, TILE), 1) - iota((heads, TILE), 0) - tp * heads
    own_length = jnp.full((heads, 1), lens[me], jnp.int32)
    decay, beta = [], []
    for t in range(NEW):
        line = small[0:1, :]
        first = 2 * all_heads * t
        scale_t = rstd[t : t + 1, :]
        alpha = jnp.sum(jnp.where(pick == first, line, 0.0), axis=1, keepdims=True) * scale_t
        write = (
            jnp.sum(jnp.where(pick == first + all_heads, line, 0.0), axis=1, keepdims=True)
            * scale_t
        )
        x = alpha + bias
        soft = jnp.maximum(x, 0.0) + jnp.log1p(jnp.exp(-jnp.abs(x)))
        live = own_length > t
        decay.append(jnp.exp(jnp.where(live, -rate * soft, 0.0)))
        beta.append(jnp.where(live, jax.nn.sigmoid(write), 0.0))
    loaded(v_mem, 9)
    total = reduce_end(total, proj_last, proj_sem)
    scale = rs_buf[...]
    for h in range(heads):
        piece = total[:, h * DV : (h + 1) * DV] * scale
        xs_buf[h * 16 : (h + 1) * 16, :] = piece.astype(BF16).astype(F32)

    def slot_rows(ref, index, stride):
        return ref[pl.ds(index, heads, stride=stride), :]

    query, key_rows, value, gate = (
        [slot_rows(xs_buf, p * NEW + t, 16) for t in range(NEW)] for p in range(4)
    )
    query = [unit_rows(x) * DK ** (-0.5) for x in query]
    key_rows = [unit_rows(x) for x in key_rows]
    for t in range(NEW):
        kq_buf[pl.ds(t, heads, stride=8), :] = key_rows[t]
        kq_buf[pl.ds(NEW + t, heads, stride=8), :] = query[t]
    for h in range(heads):
        r_buf[h * 8 : (h + 1) * 8, :] = dot(kq_buf[h * 8 : (h + 1) * 8, :], v_mem[h], HIGH)
    seen_k = [slot_rows(r_buf, t, 8) for t in range(NEW)]
    seen_q = [slot_rows(r_buf, NEW + t, 8) for t in range(NEW)]

    def inner(a, b):
        return jnp.sum(a * b, axis=1, keepdims=True)

    corrections = []
    for t in range(NEW):
        for r in range(t, NEW):
            seen_k[r] = seen_k[r] * decay[t]
            seen_q[r] = seen_q[r] * decay[t]
        fix = beta[t] * (value[t] - seen_k[t])
        corrections.append(fix)
        for r in range(t, NEW):
            if r > t:
                seen_k[r] = seen_k[r] + inner(key_rows[t], key_rows[r]) * fix
            seen_q[r] = seen_q[r] + inner(key_rows[t], query[r]) * fix
    for t in range(NEW):
        o = seen_q[t]
        o = o * lax.rsqrt(jnp.mean(o * o, axis=1, keepdims=True) + epsilon)
        o = o * head_gain[...] * (gate[t] * jax.nn.sigmoid(gate[t]))
        mix_buf[pl.ds(t, heads, stride=NEW), :] = o
    mix_all[me] = mix_buf[...].astype(BF16)

    @pl.loop(1, kv_count)
    def _(off):
        to = lax.rem(me + off, kv_count)
        remote(mix_all.at[me], mix_all.at[me], 4, mix_sem, to).start()

    u_buf[...] = jnp.zeros_like(u_buf)
    after = jnp.ones((heads, 1), F32)
    for t in range(NEW - 1, -1, -1):
        u_buf[pl.ds(t, heads, stride=8), :] = corrections[t] * after
        after = after * decay[t]
    a_buf[...] = jnp.broadcast_to(after, (heads, TILE))
    for h in range(heads):
        outer = lax.dot_general(
            kq_buf[h * 8 : (h + 1) * 8, :],
            u_buf[h * 8 : (h + 1) * 8, :],
            (((0,), (0,)), ((), ())),
            precision=HIGH,
            preferred_element_type=F32,
        )
        v_mem[h] = v_mem[h] * a_buf[h : h + 1, :] + outer
    loaded(v_output, 10)
    loaded(v_gu, 11)
    loaded(v_down, 12)

    arrived(mix_all.at[pl.ds(0, kv_count - 1)], mix_sem)
    gathered = mix_all[...].reshape(slots_wide, DV)
    packed = dot(collect, gathered).astype(BF16)
    packed = jnp.concatenate(
        [packed[h * compact : (h + 1) * compact, :] for h in range(heads)], axis=1
    )
    attended = tp_swap(0, dot(packed, v_output[...]))
    hidden = (tok_packed + attended).astype(BF16).astype(F32)
    squares = jnp.sum(hidden * hidden, axis=1, keepdims=True)
    spot = (iota((compact, TILE), 0) & (GROUP - 1)) == iota((compact, TILE), 1)
    squares = jnp.sum(jnp.where(spot, squares, 0.0).reshape(groups, GROUP, TILE), axis=1)
    sq_send[...] = squares.reshape(groups, 1, TILE)
    sq_recv[me] = sq_send[group_me]

    @pl.loop(1, kv_count)
    def _(off):
        to = lax.rem(me + off, kv_count)
        remote(sq_send.at[lax.rem(to, groups)], sq_recv.at[me], 5, sq_sem, to).start()

    hscaled = hidden * mlp_gain[...]
    blank = jnp.zeros((GROUP, width), F32)
    gate_rows, up_rows = [], []
    for g in range(groups):
        own = hscaled[g * GROUP : (g + 1) * GROUP, :]
        gate_rows += [own, blank]
        up_rows += [blank, own]
    gate_rows = jnp.concatenate(gate_rows, axis=0).astype(BF16)
    up_rows = jnp.concatenate(up_rows, axis=0).astype(BF16)
    for step in steps:
        zone = zone_of(step)
        cols = pl.ds(pl.multiple_of(zone * chunk, TILE), chunk)
        term = dot(gate_rows, v_gu[0, :, cols]) + dot(up_rows, v_gu[1, :, cols])
        gu_send[pl.ds(zone * groups, groups)] = term.astype(BF16).reshape(
            groups, 2 * GROUP, chunk
        )
        send_plane(gu_send, gu_recv, 6, gu_sem, zone)
    both = reduce_start(gu_send, gu_recv, gu_part, gu_last, gu_sem, 7, mlp_sem)
    arrived(sq_recv.at[pl.ds(0, kv_count - 1)], sq_sem)
    mean_sq = jnp.sum(sq_recv[...].reshape(kv_count, TILE), axis=0, keepdims=True)
    spot = iota((GROUP, TILE), 0) == iota((GROUP, TILE), 1)
    mean_sq = jnp.sum(jnp.where(spot, mean_sq, 0.0), axis=1, keepdims=True)
    rstd2 = lax.rsqrt(mean_sq / total_width + epsilon)
    both = reduce_end(both, gu_last, mlp_sem)
    gated = both[:GROUP] * rstd2
    active = gated * jax.nn.sigmoid(gated) * (both[GROUP:] * rstd2)
    act_all[me] = active.astype(BF16)

    def pass_on(zone, arrival, partner):
        block = zone * groups + group_me
        remote(act_all.at[block], act_all.at[block], 8, arrival, partner).start()

    def forward(zone):
        for g in range(1, groups):
            pass_on(zone, far_sem + zone, zone_me * groups + peer(g))

    for step in steps[:-1]:
        pass_on(zone_me, near_sem + zone_me, zone_of(step) * groups + group_me)
    forward(zone_me)
    near_first = steps[::-1]
    for step in near_first[1:]:
        zone = zone_of(step)
        arrived(act_all.at[zone * groups + group_me], near_sem + zone)
        forward(zone)
    feed = jnp.zeros((compact, width), F32)
    for step in near_first:
        zone = zone_of(step)
        arrived(act_all.at[pl.ds(zone * groups, groups - 1)], far_sem + zone)
        part = act_all[pl.ds(zone * groups, groups)].astype(F32).reshape(compact, chunk)
        cols = pl.ds(pl.multiple_of(zone * chunk, TILE), chunk)
        feed = feed + dot(part.astype(BF16), v_down[cols, :])

    def drain():
        left(small_send.at[pl.ds(0, groups - 1)], 0)
        left(proj_send.at[pl.ds(0, kv_count - zones)], 1)
        left(small_part.at[pl.ds(0, zones - 1)], 2)
        left(proj_part.at[pl.ds(0, zones - 1)], 3)
        left(mix_all.at[pl.ds(0, kv_count - 1)], 4)
        left(sq_recv.at[pl.ds(0, kv_count - 1)], 5)
        left(gu_send.at[pl.ds(0, kv_count - zones)], 6)
        left(gu_part.at[pl.ds(0, zones - 1)], 7)
        left(act_all.at[pl.ds(0, kv_count - 1)], 8)

    result = (hidden + tp_swap(1, feed, drain)).astype(BF16)
    out[...] = dot(unpack, result).astype(BF16)


def fused_device(
    tokens,
    lengths,
    memory,
    norm_gain,
    w_query,
    w_key,
    w_value,
    w_outgate,
    w_alpha,
    w_beta,
    decay_log,
    decay_bias,
    head_gain,
    w_output,
    mlp_gain,
    w_gate,
    w_up,
    w_down,
):
    kv_count = lax.axis_size("kv")
    rows, width = tokens.shape
    heads = memory.shape[1]
    all_heads = w_alpha.shape[1]
    live_rows = (rows // NEW) * 7 // 4
    compact = -(-live_rows // 16) * 16
    groups = compact // GROUP
    zones = kv_count // groups
    chunk = w_gate.shape[1] // zones
    wide = heads * DV
    near = pl.BlockSpec(memory_space=pltpu.VMEM)
    far = pl.BlockSpec(memory_space=pltpu.HBM)
    out, state = pl.pallas_call(
        fused,
        out_shape=(
            jax.ShapeDtypeStruct((rows, width), BF16),
            jax.ShapeDtypeStruct(memory.shape[1:], F32),
        ),
        in_specs=[far] * 18,
        out_specs=(near, near),
        scratch_shapes=[
            pltpu.SMEM(lengths.shape, jnp.int32),
            pltpu.VMEM((rows, width), BF16),
            pltpu.VMEM((1, width), F32),
            pltpu.VMEM((2, 1, heads), F32),
            pltpu.VMEM((1, DV), F32),
            pltpu.VMEM((1, width), F32),
            pltpu.VMEM((2, all_heads, width), BF16),
            pltpu.VMEM((4, *w_query.shape), BF16),
            pltpu.VMEM(w_output.shape, BF16),
            pltpu.VMEM((2, *w_gate.shape), BF16),
            pltpu.VMEM(w_down.shape, BF16),
            pltpu.VMEM((kv_count, 16, wide), BF16),
            pltpu.VMEM((kv_count, 16, wide), BF16),
            pltpu.VMEM((zones, 16, wide), BF16),
            pltpu.VMEM((zones, 16, wide), BF16),
            pltpu.VMEM((groups, zones, 2, TILE), F32),
            pltpu.VMEM((groups, zones, 2, TILE), F32),
            pltpu.VMEM((zones, 2, TILE), F32),
            pltpu.VMEM((zones, 2, TILE), F32),
            pltpu.VMEM((16, TILE), F32),
            pltpu.VMEM((heads * 16, TILE), F32),
            pltpu.VMEM((heads * 8, TILE), F32),
            pltpu.VMEM((heads * 8, TILE), F32),
            pltpu.VMEM((heads * 8, TILE), F32),
            pltpu.VMEM((heads, TILE), F32),
            pltpu.VMEM((heads * NEW, TILE), F32),
            pltpu.VMEM((kv_count, heads * NEW, TILE), BF16),
            pltpu.VMEM((2, compact, width), F32),
            pltpu.VMEM((2, compact, width), F32),
            pltpu.VMEM((groups, 1, TILE), F32),
            pltpu.VMEM((kv_count, 1, TILE), F32),
            pltpu.VMEM((kv_count, 2 * GROUP, chunk), BF16),
            pltpu.VMEM((kv_count, 2 * GROUP, chunk), BF16),
            pltpu.VMEM((zones, 2 * GROUP, chunk), BF16),
            pltpu.VMEM((zones, 2 * GROUP, chunk), BF16),
            pltpu.VMEM((kv_count, GROUP, chunk), BF16),
            pltpu.SemaphoreType.DMA((13,)),
            pltpu.SemaphoreType.DMA((9,)),
            pltpu.SemaphoreType.DMA((4 * zones + 6,)),
            pltpu.SemaphoreType.DMA((2, 2)),
        ],
        compiler_params=pltpu.CompilerParams(
            collective_id=0, has_side_effects=True, vmem_limit_bytes=48 * 1024 * 1024
        ),
    )(*[pltpu.with_memory_space_constraint(x, pltpu.HBM) for x in (
        lengths,
        tokens,
        norm_gain.reshape(1, -1),
        decay_log.reshape(1, -1),
        decay_bias.reshape(1, -1),
        head_gain.reshape(1, -1),
        mlp_gain.reshape(1, -1),
        w_alpha.T,
        w_beta.T,
        memory.reshape(memory.shape[1:]),
        w_query,
        w_key,
        w_value,
        w_outgate,
        w_output,
        w_gate,
        w_up,
        w_down,
    )])
    return out, state.reshape(memory.shape)


def fits(tokens, memory, w_alpha, w_gate):
    kv_count = lax.axis_size("kv")
    rows, width = tokens.shape
    live_rows = (rows // NEW) * 7 // 4
    groups = -(-live_rows // 16) * 16 // GROUP
    all_heads = w_alpha.shape[1]
    return (
        lax.axis_size("tp") == 2
        and memory.shape[0] == 1
        and memory.shape[1] == 8
        and rows == kv_count * NEW
        and rows % 16 == 0
        and width % TILE == 0
        and kv_count % groups == 0
        and w_gate.shape[1] % (kv_count // groups * TILE) == 0
        and NEW * 2 * all_heads == TILE
    )


def layer(*arrays):
    if fits(arrays[0], arrays[2], arrays[8], arrays[15]):
        return fused_device(*arrays)
    return per_device(*arrays)


def solution(mesh):
    placed = (
        P(None, "kv"),
        P(),
        P("kv", "tp", None, None),
        P("kv"),
        P("kv", "tp"),
        P("kv", "tp"),
        P("kv", "tp"),
        P("kv", "tp"),
        P("kv", None),
        P("kv", None),
        P("tp"),
        P("tp"),
        P(),
        P("tp", "kv"),
        P("kv"),
        P("kv", "tp"),
        P("kv", "tp"),
        P("tp", "kv"),
    )
    return jax.shard_map(
        layer,
        mesh=mesh,
        in_specs=placed,
        out_specs=(P(None, "kv"), P("kv", "tp", None, None)),
        check_vma=False,
    )
```

```python
import jax
import jax.numpy as jnp
from jax import lax
from jax.experimental import pallas as pl
from jax.experimental.pallas import tpu as pltpu
from jax.sharding import PartitionSpec as P

D = 4096
DK = 128
DV = 128
NEW = 4


epsilon = 1e-06


def unit_rows(values):
    return values * lax.rsqrt(jnp.sum(values * values, axis=-1, keepdims=True) + epsilon)


def advance(memory, queries, key_rows, value_rows, decays, betas):
    outputs = []
    for step in range(queries.shape[1]):
        memory = jnp.exp(decays[:, step])[:, :, None, None] * memory
        predicted = jnp.einsum(
            "shde,shd->she", memory, key_rows[:, step], precision=lax.Precision.HIGHEST
        )
        correction = betas[:, step][:, :, None] * (value_rows[:, step] - predicted)
        memory = memory + key_rows[:, step][:, :, :, None] * correction[:, :, None, :]
        outputs.append(
            jnp.einsum("shde,shd->she", memory, queries[:, step], precision=lax.Precision.HIGHEST)
        )
    return (memory, jnp.stack(outputs, axis=1))


def per_device(
    tokens,
    lengths,
    memory,
    norm_gain,
    w_query,
    w_key,
    w_value,
    w_outgate,
    w_alpha,
    w_beta,
    decay_log,
    decay_bias,
    head_gain,
    w_output,
    mlp_gain,
    w_gate,
    w_up,
    w_down,
):
    total_rows = tokens.shape[0]
    kv_count = lax.axis_size("kv")
    kv_place = lax.axis_index("kv")
    tp_place = lax.axis_index("tp")
    own_rows = total_rows // kv_count
    seq_dev = memory.shape[0]
    heads_dev = memory.shape[1]
    token_f = tokens.astype(jnp.float32)
    squares = jnp.sum(token_f * token_f, axis=1)
    scaled = (token_f * norm_gain).astype(jnp.bfloat16)
    part_query = jnp.dot(scaled, w_query, preferred_element_type=jnp.float32)
    part_key = jnp.dot(scaled, w_key, preferred_element_type=jnp.float32)
    part_value = jnp.dot(scaled, w_value, preferred_element_type=jnp.float32)
    part_gate = jnp.dot(scaled, w_outgate, preferred_element_type=jnp.float32)
    part_alpha = jnp.dot(scaled, w_alpha, preferred_element_type=jnp.float32)
    part_beta = jnp.dot(scaled, w_beta, preferred_element_type=jnp.float32)
    all_squares = lax.psum(squares, "kv")
    sum_query, sum_key, sum_value, sum_gate, sum_alpha, sum_beta = (
        lax.psum_scatter(part_query, "kv", scatter_dimension=0, tiled=True),
        lax.psum_scatter(part_key, "kv", scatter_dimension=0, tiled=True),
        lax.psum_scatter(part_value, "kv", scatter_dimension=0, tiled=True),
        lax.psum_scatter(part_gate, "kv", scatter_dimension=0, tiled=True),
        lax.psum_scatter(part_alpha, "kv", scatter_dimension=0, tiled=True),
        lax.psum_scatter(part_beta, "kv", scatter_dimension=0, tiled=True),
    )
    own_squares = lax.dynamic_slice_in_dim(all_squares, kv_place * own_rows, own_rows)
    rstd = lax.rsqrt(own_squares / D + epsilon)[:, None]
    queries = (sum_query * rstd).astype(jnp.bfloat16)
    key_rows = (sum_key * rstd).astype(jnp.bfloat16)
    value_rows = (sum_value * rstd).astype(jnp.bfloat16)
    outgate = (sum_gate * rstd).astype(jnp.bfloat16)
    alphas = lax.dynamic_slice_in_dim(sum_alpha * rstd, tp_place * heads_dev, heads_dev, 1)
    beta_pre = lax.dynamic_slice_in_dim(sum_beta * rstd, tp_place * heads_dev, heads_dev, 1)
    own_lengths = lax.dynamic_slice_in_dim(lengths, kv_place * seq_dev, seq_dev)
    live = jnp.arange(NEW, dtype=jnp.int32)[None, :] < own_lengths[:, None]
    query_h = unit_rows(queries.astype(jnp.float32).reshape(seq_dev, NEW, heads_dev, DK)) * DK ** (
        -0.5
    )
    key_h = unit_rows(key_rows.astype(jnp.float32).reshape(seq_dev, NEW, heads_dev, DK))
    value_h = value_rows.astype(jnp.float32).reshape(seq_dev, NEW, heads_dev, DV)
    decays = -jnp.exp(decay_log) * jax.nn.softplus(alphas + decay_bias)
    decays = jnp.where(live[:, :, None], decays.reshape(seq_dev, NEW, heads_dev), 0.0)
    betas = jnp.where(
        live[:, :, None], jax.nn.sigmoid(beta_pre).reshape(seq_dev, NEW, heads_dev), 0.0
    )
    new_memory, attended = advance(memory, query_h, key_h, value_h, decays, betas)
    attended = attended * lax.rsqrt(jnp.mean(attended * attended, axis=-1, keepdims=True) + epsilon)
    gate_h = outgate.astype(jnp.float32).reshape(seq_dev, NEW, heads_dev, DV)
    mixed = (
        (attended * head_gain * jax.nn.silu(gate_h))
        .astype(jnp.bfloat16)
        .reshape(own_rows, heads_dev * DV)
    )
    attn_terms = jnp.dot(
        lax.all_gather(mixed, "kv", axis=0, tiled=True),
        w_output,
        preferred_element_type=jnp.float32,
    )
    attn_total = lax.psum(attn_terms, "tp")
    hidden = (token_f + attn_total).astype(jnp.bfloat16)
    hidden_f = hidden.astype(jnp.float32)
    hidden_squares = jnp.sum(hidden_f * hidden_f, axis=1)
    hscaled = (hidden_f * mlp_gain).astype(jnp.bfloat16)
    all_live = (jnp.arange(NEW, dtype=jnp.int32)[None, :] < lengths[:, None]).reshape(total_rows)
    part_gate_rows = jnp.dot(hscaled, w_gate, preferred_element_type=jnp.float32)
    part_up_rows = jnp.dot(hscaled, w_up, preferred_element_type=jnp.float32)
    gate_rows, up_rows, mlp_squares = lax.psum((part_gate_rows, part_up_rows, hidden_squares), "kv")
    rstd2 = lax.rsqrt(mlp_squares / D + epsilon)[:, None]
    active = (jax.nn.silu(gate_rows * rstd2) * (up_rows * rstd2)).astype(jnp.bfloat16)
    feed_terms = jnp.dot(active, w_down, preferred_element_type=jnp.float32)
    feed_total = lax.psum(feed_terms.astype(jnp.bfloat16), "tp").astype(jnp.float32)
    layer_out = jnp.where(all_live[:, None], hidden_f + feed_total, 0.0).astype(jnp.bfloat16)
    return (layer_out, new_memory)


F32 = jnp.float32
BF16 = jnp.bfloat16
HIGH = lax.Precision.HIGHEST
TILE = 128
GROUP = 8


def iota(shape, axis):
    return lax.broadcasted_iota(jnp.int32, shape, axis)


def dot(a, b, precision=None):
    return jnp.dot(a, b, preferred_element_type=F32, precision=precision)


def fused(
    lens_far,
    tokens_far,
    norm_far,
    decay_log_far,
    decay_bias_far,
    head_far,
    mlp_far,
    alpha_far,
    beta_far,
    memory,
    w_query,
    w_key,
    w_value,
    w_outgate,
    w_output,
    w_gate,
    w_up,
    w_down,
    out,
    v_mem,
    lens,
    tokens,
    norm_gain,
    decay_in,
    head_gain,
    mlp_gain,
    v_ab,
    v_proj,
    v_output,
    v_gu,
    v_down,
    proj_send,
    proj_recv,
    proj_part,
    proj_last,
    small_send,
    small_recv,
    small_part,
    small_last,
    rs_buf,
    xs_buf,
    kq_buf,
    r_buf,
    u_buf,
    a_buf,
    mix_buf,
    mix_all,
    tp_send,
    tp_recv,
    sq_send,
    sq_recv,
    gu_send,
    gu_recv,
    gu_part,
    gu_last,
    act_all,
    load_sem,
    send_sem,
    recv_sem,
    tp_sem,
):
    kv_count = mix_all.shape[0]
    me = lax.axis_index("kv")
    tp = lax.axis_index("tp")
    rows, width = tokens.shape
    heads = v_mem.shape[0]
    wide = heads * DV
    compact = tp_send.shape[1]
    groups = compact // GROUP
    zones = kv_count // groups
    sent = gu_send.shape[2]
    chunk = sent + TILE
    held = GROUP - 1
    total_width = width * kv_count
    all_heads = v_ab.shape[1]
    zone_me = me // groups
    group_me = lax.rem(me, groups)
    steps = [*range(1, zones), 0]
    side, odd = zone_me // 2, lax.rem(zone_me, 2)

    def zone_of(step):
        if zones != 4:
            return lax.rem(zone_me + step, zones)
        across = (1 - side) * 2
        return [zone_me, across + 1 - odd, across + odd, side * 2 + 1 - odd][step]

    def peer(g):
        if groups != 4:
            return lax.rem(group_me + g, groups)
        row, col = group_me // 2, lax.rem(group_me, 2)
        return [
            group_me,
            (1 - row) * 2 + 1 - col,
            row * 2 + 1 - col,
            (1 - row) * 2 + col,
        ][g]

    barrier = pltpu.get_barrier_semaphore()

    def greet(**where):
        pl.semaphore_signal(
            barrier, inc=1, device_id=where, device_id_type=pl.DeviceIdType.MESH
        )

    for core in (tp, 1 - tp):
        for g in range(1, groups):
            greet(kv=zone_me * groups + peer(g), tp=core)
        for step in steps[:-1]:
            greet(kv=zone_of(step) * groups + group_me, tp=core)
    greet(tp=1 - tp)

    def load(src, dst, sem):
        return pltpu.make_async_copy(src, dst, load_sem.at[sem])

    half = wide // 2
    halves = [slice(c * half, (c + 1) * half) for c in range(2)]
    load(tokens_far, tokens, 0).start()
    load(norm_far, norm_gain, 1).start()
    load(alpha_far, v_ab.at[0], 2).start()
    load(beta_far, v_ab.at[1], 2).start()
    for c in range(2):
        for p, weight in enumerate((w_query, w_key, w_value, w_outgate)):
            load(weight.at[:, halves[c]], v_proj.at[p, :, halves[c]], 3 + c).start()
    load(lens_far, lens, 5).start()
    load(decay_log_far, decay_in.at[0], 6).start()
    load(decay_bias_far, decay_in.at[1], 6).start()
    load(head_far, head_gain, 7).start()
    load(mlp_far, mlp_gain, 8).start()

    def loaded(ref, sem):
        load(ref, ref, sem).wait()

    plane_sem, gu_sem, near_sem, far_sem = 0, zones, 3 * zones, 5 * zones
    proj_sem, mlp_sem, mix_sem, small_sem, few_sem, sq_sem = range(6 * zones, 6 * zones + 6)
    both_sem = 6 * zones + 6

    def remote(src, dst, sent, arrival, partner, core=None):
        return pltpu.make_async_remote_copy(
            src_ref=src,
            dst_ref=dst,
            send_sem=send_sem.at[sent],
            recv_sem=recv_sem.at[arrival],
            device_id={"kv": partner, "tp": tp if core is None else core},
            device_id_type=pl.DeviceIdType.MESH,
        )

    def arrived(ref, arrival):
        remote(ref, ref, 0, arrival, me).wait_recv()

    def left(ref, sent):
        remote(ref, ref, sent, 0, me).wait_send()

    def tp_swap(phase, value, meanwhile=None):
        tp_send[phase] = value
        swap = pltpu.make_async_remote_copy(
            src_ref=tp_send.at[phase],
            dst_ref=tp_recv.at[phase],
            send_sem=tp_sem.at[phase, 0],
            recv_sem=tp_sem.at[phase, 1],
            device_id={"tp": 1 - tp},
            device_id_type=pl.DeviceIdType.MESH,
        )
        swap.start()
        if meanwhile is not None:
            meanwhile()
        swap.wait()
        return value + tp_recv[phase]

    packed_rows = kv_count * 2 * NEW
    row = iota((packed_rows, rows), 0)
    spread = jnp.where(
        iota((packed_rows, rows), 1) == (row >> 3) * NEW + (row & 3), 1.0, 0.0
    ).astype(BF16)
    seq_row = iota((kv_count, rows), 0)
    seq_row = lax.rem(seq_row, zones) * groups + seq_row // zones
    lane = iota((kv_count, TILE), 1)
    place = iota((TILE, all_heads), 0) & (2 * all_heads - 1)
    head_of = iota((TILE, all_heads), 1)
    one_alpha = jnp.where(place == head_of, 1.0, 0.0).astype(BF16)
    one_beta = jnp.where(place == head_of + all_heads, 1.0, 0.0).astype(BF16)
    loaded(tokens, 0)
    loaded(norm_gain, 1)
    tok = tokens[...]
    scaled = (tok.astype(F32) * norm_gain[...]).astype(BF16)
    wide_scaled = dot(spread, scaled)
    part_of = iota((packed_rows, width), 0) & 7
    low = jnp.where(part_of < NEW, wide_scaled, 0.0).astype(BF16)
    high = jnp.where(part_of >= NEW, wide_scaled, 0.0).astype(BF16)

    def sum_plane(recv, sem, first, own):
        count = groups if own is None else groups - 1
        arrived(recv.at[pl.ds(first, count)], sem)
        added = (recv[first + group_me] if own is None else own).astype(F32)
        for g in range(1, groups):
            added = added + recv[first + peer(g)].astype(F32)
        return added

    def send_proj(zone, cols=slice(0, wide)):
        def send(slab, place, partner):
            remote(
                proj_send.at[slab, :, cols],
                proj_recv.at[place, :, cols],
                1,
                plane_sem + zone,
                partner,
                1 - tp,
            ).start()

        for g in range(1, groups):
            send(
                zone * groups + peer(g),
                zone * groups + group_me,
                zone_me * groups + peer(g),
            )
        send(zone * groups + group_me, zone * groups + group_me, me)

    for c in range(2):
        loaded(v_proj.at[:, :, halves[c]], 3 + c)
        parts = [
            dot(low, v_proj[p, :, halves[c]]) + dot(high, v_proj[p + 1, :, halves[c]])
            for p in (0, 2)
        ]
        parts = [part.reshape(kv_count, 2 * NEW, half) for part in parts]
        proj_send[:, :, halves[c]] = jnp.concatenate(parts, axis=1).astype(BF16)
        if c == 0:
            pl.semaphore_wait(barrier, 2 * (groups + zones - 2) + 1)
        send_proj(zone_of(steps[0]), halves[c])
    load(memory, v_mem, 9).start()
    load(w_output, v_output, 10).start()
    load(w_gate, v_gu.at[0], 11).start()
    load(w_up, v_gu.at[1], 11).start()
    load(w_down, v_down, 12).start()
    loaded(v_ab, 2)
    w_small = (dot(one_alpha, v_ab[0]) + dot(one_beta, v_ab[1])).astype(BF16)
    small = jnp.zeros((kv_count, TILE), F32)
    squares = jnp.zeros((kv_count, TILE), F32)
    for t in range(NEW):
        take = jnp.where(iota((kv_count, rows), 1) == seq_row * NEW + t, 1.0, 0.0).astype(BF16)
        took = lax.dot_general(
            dot(take, scaled).astype(BF16),
            w_small,
            (((1,), (1,)), ((), ())),
            preferred_element_type=F32,
        )
        small = jnp.where(lane // (2 * all_heads) == t, took, small)
        tok_t = dot(take, tok)
        squares = jnp.where(
            lane == t, jnp.sum(tok_t * tok_t, axis=1, keepdims=True), squares
        )
    small_send[:, :, 0, :] = small.reshape(groups, zones, TILE)
    small_send[:, :, 1, :] = squares.reshape(groups, zones, TILE)
    for g in range(1, groups):
        remote(
            small_send.at[peer(g)],
            small_recv.at[group_me],
            0,
            small_sem,
            zone_me * groups + peer(g),
        ).start()
    for step in steps[1:-1]:
        send_proj(zone_of(step))
    for g in range(1, groups):
        remote(
            proj_send.at[zone_me * groups + peer(g)],
            proj_recv.at[me],
            1,
            plane_sem + zone_me,
            zone_me * groups + peer(g),
        ).start()

    loaded(lens, 5)
    loaded(decay_in, 6)
    loaded(head_gain, 7)
    loaded(mlp_gain, 8)
    slots_wide = kv_count * heads * NEW
    shape_a = (1, rows)
    shape_b = (1, slots_wide)
    shape_c = (rows, compact)
    length_a = jnp.zeros(shape_a, jnp.int32)
    start_a = jnp.zeros(shape_a, jnp.int32)
    length_b = jnp.zeros(shape_b, jnp.int32)
    start_b = jnp.zeros(shape_b, jnp.int32)
    length_c = jnp.zeros(shape_c, jnp.int32)
    start_c = jnp.zeros(shape_c, jnp.int32)
    seq_a = iota(shape_a, 1) >> 2
    seq_b = iota(shape_b, 1) >> 5
    seq_c = iota(shape_c, 0) >> 2
    begin = jnp.int32(0)
    for s in range(kv_count):
        length_a = jnp.where(seq_a == s, lens[s], length_a)
        start_a = jnp.where(seq_a == s, begin, start_a)
        length_b = jnp.where(seq_b == s, lens[s], length_b)
        start_b = jnp.where(seq_b == s, begin, start_b)
        length_c = jnp.where(seq_c == s, lens[s], length_c)
        start_c = jnp.where(seq_c == s, begin, start_c)
        begin = begin + lens[s]
    slot_a = iota(shape_a, 1) & 3

    def padded(rank):
        return sum(((rank >= g * held).astype(jnp.int32) for g in range(1, groups)), rank)

    rank_a = jnp.where(slot_a < length_a, padded(start_a + slot_a), -1)
    pack = jnp.where(rank_a == iota((compact, rows), 0), 1.0, 0.0).astype(BF16)
    slot_c = iota(shape_c, 0) & 3
    rank_c = jnp.where(slot_c < length_c, padded(start_c + slot_c), -1)
    unpack = jnp.where(rank_c == iota(shape_c, 1), 1.0, 0.0).astype(BF16)
    slot_b = iota(shape_b, 1) & 3
    head_b = (iota(shape_b, 1) >> 2) & (heads - 1)
    rank_b = jnp.where(slot_b < length_b, head_b * compact + padded(start_b + slot_b), -1)
    collect = jnp.where(rank_b == iota((heads * compact, slots_wide), 0), 1.0, 0.0).astype(BF16)
    tok_packed = dot(pack, tok)

    def proj_onward(zone):
        proj_part[zone] = sum_plane(proj_recv, plane_sem + zone, zone * groups, None).astype(BF16)
        remote(
            proj_part.at[zone],
            proj_last.at[zone_me],
            3,
            proj_sem,
            zone * groups + group_me,
            1 - tp,
        ).start()

    proj_onward(zone_of(steps[0]))
    arrived(small_recv.at[pl.ds(0, groups - 1)], small_sem)
    small = small_send[group_me]
    for g in range(1, groups):
        small = small + small_recv[peer(g)]
    small_part[...] = small
    for step in steps[:-1]:
        zone = zone_of(step)
        remote(
            small_part.at[zone], small_last.at[zone_me], 2, few_sem, zone * groups + group_me
        ).start()

    for step in steps[1:-1]:
        proj_onward(zone_of(step))
    total = sum_plane(proj_recv, plane_sem + zone_me, zone_me * groups, proj_send[me])
    arrived(small_last.at[pl.ds(0, zones - 1)], few_sem)
    small = small_part[zone_me]
    for step in steps[:-1]:
        small = small + small_last[zone_of(step)]
    diagonal = iota((NEW, TILE), 0) == iota((NEW, TILE), 1)
    mean_sq = jnp.sum(jnp.where(diagonal, small[1:2, :], 0.0), axis=1, keepdims=True)
    rstd = lax.rsqrt(mean_sq / total_width + epsilon)
    rstd_wide = jnp.broadcast_to(rstd, (NEW, TILE))
    for p in range(4):
        rs_buf[p * NEW : (p + 1) * NEW, :] = rstd_wide
    eye = iota((heads, heads), 0) == iota((heads, heads), 1)
    rate = jnp.sum(jnp.where(eye, jnp.exp(decay_in[0]), 0.0), axis=1, keepdims=True)
    bias = jnp.sum(jnp.where(eye, decay_in[1], 0.0), axis=1, keepdims=True)
    pick = iota((heads, TILE), 1) - iota((heads, TILE), 0) - tp * heads
    own_length = jnp.full((heads, 1), lens[me], jnp.int32)
    decay, beta = [], []
    for t in range(NEW):
        line = small[0:1, :]
        first = 2 * all_heads * t
        scale_t = rstd[t : t + 1, :]
        alpha = jnp.sum(jnp.where(pick == first, line, 0.0), axis=1, keepdims=True) * scale_t
        write = (
            jnp.sum(jnp.where(pick == first + all_heads, line, 0.0), axis=1, keepdims=True)
            * scale_t
        )
        x = alpha + bias
        soft = jnp.maximum(x, 0.0) + jnp.log1p(jnp.exp(-jnp.abs(x)))
        live = own_length > t
        decay.append(jnp.exp(jnp.where(live, -rate * soft, 0.0)))
        beta.append(jnp.where(live, jax.nn.sigmoid(write), 0.0))
    loaded(v_mem, 9)
    arrived(proj_last.at[pl.ds(0, zones - 1)], proj_sem)
    for step in steps[:-1]:
        total = total + proj_last[zone_of(step)].astype(F32)
    scale = rs_buf[...]
    for h in range(heads):
        piece = total[:, h * DV : (h + 1) * DV] * scale
        xs_buf[h * 16 : (h + 1) * 16, :] = piece.astype(BF16).astype(F32)

    def slot_rows(ref, index, stride):
        return ref[pl.ds(index, heads, stride=stride), :]

    query, key_rows, value, gate = (
        [slot_rows(xs_buf, p * NEW + t, 16) for t in range(NEW)] for p in range(4)
    )
    query = [unit_rows(x) * DK ** (-0.5) for x in query]
    key_rows = [unit_rows(x) for x in key_rows]
    for t in range(NEW):
        kq_buf[pl.ds(t, heads, stride=8), :] = key_rows[t]
        kq_buf[pl.ds(NEW + t, heads, stride=8), :] = query[t]
    for h in range(heads):
        r_buf[h * 8 : (h + 1) * 8, :] = dot(kq_buf[h * 8 : (h + 1) * 8, :], v_mem[h], HIGH)
    seen_k = [slot_rows(r_buf, t, 8) for t in range(NEW)]
    seen_q = [slot_rows(r_buf, NEW + t, 8) for t in range(NEW)]

    def inner(a, b):
        return jnp.sum(a * b, axis=1, keepdims=True)

    corrections = []
    for t in range(NEW):
        for r in range(t, NEW):
            seen_k[r] = seen_k[r] * decay[t]
            seen_q[r] = seen_q[r] * decay[t]
        fix = beta[t] * (value[t] - seen_k[t])
        corrections.append(fix)
        for r in range(t, NEW):
            if r > t:
                seen_k[r] = seen_k[r] + inner(key_rows[t], key_rows[r]) * fix
            seen_q[r] = seen_q[r] + inner(key_rows[t], query[r]) * fix
    for t in range(NEW):
        o = seen_q[t]
        o = o * lax.rsqrt(jnp.mean(o * o, axis=1, keepdims=True) + epsilon)
        o = o * head_gain[...] * (gate[t] * jax.nn.sigmoid(gate[t]))
        mix_buf[pl.ds(t, heads, stride=NEW), :] = o
    mix_all[me] = mix_buf[...].astype(BF16)

    def send_mix():
        for step in steps:
            for g in [*range(1, groups), 0]:
                if step or g:
                    to = zone_of(step) * groups + peer(g)
                    remote(mix_all.at[me], mix_all.at[me], 4, mix_sem, to).start()

    pl.when(tp == 0)(send_mix)
    u_buf[...] = jnp.zeros_like(u_buf)
    after = jnp.ones((heads, 1), F32)
    for t in range(NEW - 1, -1, -1):
        u_buf[pl.ds(t, heads, stride=8), :] = corrections[t] * after
        after = after * decay[t]
    a_buf[...] = jnp.broadcast_to(after, (heads, TILE))
    for h in range(heads):
        outer = lax.dot_general(
            kq_buf[h * 8 : (h + 1) * 8, :],
            u_buf[h * 8 : (h + 1) * 8, :],
            (((0,), (0,)), ((), ())),
            precision=HIGH,
            preferred_element_type=F32,
        )
        v_mem[h] = v_mem[h] * a_buf[h : h + 1, :] + outer
    pl.when(tp == 1)(send_mix)
    loaded(v_output, 10)
    loaded(v_gu, 11)
    loaded(v_down, 12)

    arrived(mix_all.at[pl.ds(0, kv_count - 1)], mix_sem)
    gathered = mix_all[...].reshape(slots_wide, DV)
    packed = dot(collect, gathered).astype(BF16)
    packed = jnp.concatenate(
        [packed[h * compact : (h + 1) * compact, :] for h in range(heads)], axis=1
    )
    attended = tp_swap(0, dot(packed, v_output[...]))
    hidden = (tok_packed + attended).astype(BF16).astype(F32)

    hscaled = hidden * mlp_gain[...]
    blank = jnp.zeros((GROUP, width), F32)
    gate_rows = []
    for g in range(groups):
        gate_rows += [hscaled[g * GROUP : (g + 1) * GROUP, :], blank]
    gate_rows = jnp.concatenate(gate_rows, axis=0)
    up_rows = pltpu.roll(gate_rows, held, 0).astype(BF16)
    gate_rows = gate_rows.astype(BF16)
    spare = (iota((2 * compact, TILE), 0) & (2 * GROUP - 1)) >= 2 * held
    for step in steps:
        zone = zone_of(step)
        cols = pl.ds(pl.multiple_of(zone * chunk, TILE), chunk)
        term = dot(gate_rows, v_gu[0, :, cols]) + dot(up_rows, v_gu[1, :, cols])
        last = term[:, sent:]
        tiles = [
            jnp.where(
                spare,
                pltpu.roll(last, 2 * (held - k), 0),
                term[:, k * TILE : (k + 1) * TILE],
            )
            for k in range(held)
        ]
        term = jnp.concatenate([*tiles, term[:, held * TILE : sent]], axis=1)
        gu_send[pl.ds(zone * groups, groups)] = term.astype(BF16).reshape(
            groups, 2 * GROUP, sent
        )
        arrival = gu_sem + tp * zones + zone
        for g in range(1, groups):
            remote(
                gu_send.at[zone * groups + peer(g)],
                gu_recv.at[tp * kv_count + zone * groups + group_me],
                6,
                arrival,
                zone_me * groups + peer(g),
                1,
            ).start()

        @pl.when(tp == 0)
        def _():
            slab = zone * groups + group_me
            remote(gu_send.at[slab], gu_recv.at[slab], 6, arrival, me, 1).start()

        if step == steps[0]:

            @pl.when(tp == 1)
            def _():
                squares = jnp.sum(hidden * hidden, axis=1, keepdims=True)
                spot = (iota((compact, TILE), 0) & (GROUP - 1)) == iota((compact, TILE), 1)
                squares = jnp.sum(jnp.where(spot, squares, 0.0).reshape(groups, GROUP, TILE), axis=1)
                sq_send[...] = squares.reshape(groups, 1, TILE)
                sq_recv[me] = sq_send[group_me]

                @pl.loop(1, kv_count)
                def _(off):
                    to = lax.rem(me + off, kv_count)
                    remote(sq_send.at[lax.rem(to, groups)], sq_recv.at[me], 5, sq_sem, to).start()

    near_first = steps[::-1]

    @pl.when(tp == 1)
    def _():
        def plane_total(zone, core):
            slab = zone * groups
            own = gu_send[slab + group_me] if core else None
            return sum_plane(gu_recv, gu_sem + core * zones + zone, core * kv_count + slab, own)

        for step in steps[:-1]:
            zone = zone_of(step)
            for core in (1, 0):
                gu_part[core * zones + zone] = plane_total(zone, core).astype(BF16)
                remote(
                    gu_part.at[core * zones + zone],
                    gu_last.at[core * zones + zone_me],
                    7,
                    mlp_sem if core else both_sem,
                    zone * groups + group_me,
                ).start()
        arrived(sq_recv.at[pl.ds(0, kv_count - 1)], sq_sem)
        mean_sq = jnp.sum(sq_recv[...].reshape(kv_count, TILE), axis=0, keepdims=True)
        spot = iota((GROUP, TILE), 0) == iota((GROUP, TILE), 1)
        mean_sq = jnp.sum(jnp.where(spot, mean_sq, 0.0), axis=1, keepdims=True)
        rstd2 = lax.rsqrt(mean_sq / total_width + epsilon)

        def pass_on(zone, core, sent, arrival, partner, there):
            block = core * kv_count + zone * groups + group_me
            remote(act_all.at[block], act_all.at[block], sent, arrival, partner, there).start()

        def forward(zone, core):
            for g in range(1, groups):
                pass_on(zone, core, 9, far_sem + zone, zone_me * groups + peer(g), core)
            if core == 0:
                pass_on(zone, 0, 9, far_sem + zone, me, 0)

        for core in (0, 1):
            both = plane_total(zone_me, core)
            arrived(
                gu_last.at[pl.ds(core * zones, zones - 1)], mlp_sem if core else both_sem
            )
            for step in steps[:-1]:
                both = both + gu_last[core * zones + zone_of(step)].astype(F32)
            row = iota((2 * GROUP, TILE), 0)
            last = jnp.zeros((2 * GROUP, TILE), F32)
            for k in range(held):
                tile = both[:, k * TILE : (k + 1) * TILE]
                back = pltpu.roll(tile, 2 * GROUP - 2 * (held - k), 0)
                last = jnp.where(row >> 1 == k, back, last)
            both = jnp.concatenate([both, last], axis=1)
            gated = both[:GROUP] * rstd2
            lifted = pltpu.roll(both, 2 * GROUP - held, 0)[:GROUP] * rstd2
            active = gated * jax.nn.sigmoid(gated) * lifted
            row = iota((GROUP, TILE), 0)
            last = active[:, sent:]
            tiles = [
                jnp.where(
                    row == held,
                    last if k == held else pltpu.roll(last, held - k, 0),
                    active[:, k * TILE : (k + 1) * TILE],
                )
                for k in range(held)
            ]
            active = jnp.concatenate([*tiles, active[:, held * TILE : sent]], axis=1)
            act_all[core * kv_count + me] = active.astype(BF16)
            for step in steps[:-1]:
                there = zone_of(step) * groups + group_me
                pass_on(zone_me, core, 8, near_sem + core * zones + zone_me, there, 1)
            forward(zone_me, core)
        for step in near_first[1:]:
            zone = zone_of(step)
            for core in (0, 1):
                block = core * kv_count + zone * groups + group_me
                arrived(act_all.at[block], near_sem + core * zones + zone)
                forward(zone, core)

    feed = jnp.zeros((compact, width), F32)
    row_in = iota((compact, TILE), 0) & (GROUP - 1)
    for step in near_first:
        zone = zone_of(step)
        first = tp * kv_count + zone * groups

        @pl.when(tp == 0)
        def _():
            arrived(act_all.at[pl.ds(first, groups)], far_sem + zone)

        @pl.when(tp == 1)
        def _():
            arrived(act_all.at[pl.ds(first, groups - 1)], far_sem + zone)

        part = act_all[pl.ds(first, groups)].astype(F32).reshape(compact, sent)
        last = jnp.zeros((compact, TILE), F32)
        for k in range(held):
            tile = part[:, k * TILE : (k + 1) * TILE]
            last = jnp.where(row_in == k, pltpu.roll(tile, compact - (held - k), 0), last)
        part = jnp.concatenate([part, last], axis=1)
        cols = pl.ds(pl.multiple_of(zone * chunk, TILE), chunk)
        feed = feed + dot(part.astype(BF16), v_down[cols, :])

    def drain():
        left(small_send.at[pl.ds(0, groups - 1)], 0)
        left(proj_send.at[pl.ds(0, kv_count - 1)], 1)
        left(small_part.at[pl.ds(0, zones - 1)], 2)
        left(proj_part.at[pl.ds(0, zones - 1)], 3)
        left(mix_all.at[pl.ds(0, kv_count - 1)], 4)

        @pl.when(tp == 0)
        def _():
            left(gu_send, 6)

        @pl.when(tp == 1)
        def _():
            left(sq_recv.at[pl.ds(0, kv_count - 1)], 5)
            left(gu_send.at[pl.ds(0, kv_count - zones)], 6)
            left(gu_part.at[pl.ds(0, 2 * (zones - 1))], 7)
            left(act_all.at[pl.ds(0, 2 * (zones - 1))], 8)
            left(act_all.at[pl.ds(0, zones * (2 * groups - 1))], 9)

    result = hidden + tp_swap(1, feed, drain)
    result = jnp.where((iota((compact, width), 0) & (GROUP - 1)) < held, result, 0.0)
    result = result.astype(BF16)
    out[...] = dot(unpack, result).astype(BF16)


def settle(out, state, out_far, state_far, sem):
    moves = [
        pltpu.make_async_copy(state, state_far, sem.at[0]),
        pltpu.make_async_copy(out, out_far, sem.at[1]),
    ]
    for move in moves:
        move.start()
    for move in moves:
        move.wait()


def fused_device(
    tokens,
    lengths,
    memory,
    norm_gain,
    w_query,
    w_key,
    w_value,
    w_outgate,
    w_alpha,
    w_beta,
    decay_log,
    decay_bias,
    head_gain,
    w_output,
    mlp_gain,
    w_gate,
    w_up,
    w_down,
):
    kv_count = lax.axis_size("kv")
    rows, width = tokens.shape
    heads = memory.shape[1]
    all_heads = w_alpha.shape[1]
    live_rows = (rows // NEW) * 7 // 4
    compact = -(-live_rows // 16) * 16
    groups = compact // GROUP
    zones = kv_count // groups
    sent = w_gate.shape[1] // zones - TILE
    wide = heads * DV
    near = pl.BlockSpec(memory_space=pltpu.VMEM)
    far = pl.BlockSpec(memory_space=pltpu.HBM)
    out, state = pl.pallas_call(
        fused,
        out_shape=(
            jax.ShapeDtypeStruct((rows, width), BF16),
            jax.ShapeDtypeStruct(memory.shape[1:], F32),
        ),
        in_specs=[far] * 18,
        out_specs=(near, near),
        scratch_shapes=[
            pltpu.SMEM(lengths.shape, jnp.int32),
            pltpu.VMEM((rows, width), BF16),
            pltpu.VMEM((1, width), F32),
            pltpu.VMEM((2, 1, heads), F32),
            pltpu.VMEM((1, DV), F32),
            pltpu.VMEM((1, width), F32),
            pltpu.VMEM((2, all_heads, width), BF16),
            pltpu.VMEM((4, *w_query.shape), BF16),
            pltpu.VMEM(w_output.shape, BF16),
            pltpu.VMEM((2, *w_gate.shape), BF16),
            pltpu.VMEM(w_down.shape, BF16),
            pltpu.VMEM((kv_count, 16, wide), BF16),
            pltpu.VMEM((kv_count, 16, wide), BF16),
            pltpu.VMEM((zones, 16, wide), BF16),
            pltpu.VMEM((zones, 16, wide), BF16),
            pltpu.VMEM((groups, zones, 2, TILE), F32),
            pltpu.VMEM((groups, zones, 2, TILE), F32),
            pltpu.VMEM((zones, 2, TILE), F32),
            pltpu.VMEM((zones, 2, TILE), F32),
            pltpu.VMEM((16, TILE), F32),
            pltpu.VMEM((heads * 16, TILE), F32),
            pltpu.VMEM((heads * 8, TILE), F32),
            pltpu.VMEM((heads * 8, TILE), F32),
            pltpu.VMEM((heads * 8, TILE), F32),
            pltpu.VMEM((heads, TILE), F32),
            pltpu.VMEM((heads * NEW, TILE), F32),
            pltpu.VMEM((kv_count, heads * NEW, TILE), BF16),
            pltpu.VMEM((2, compact, width), F32),
            pltpu.VMEM((2, compact, width), F32),
            pltpu.VMEM((groups, 1, TILE), F32),
            pltpu.VMEM((kv_count, 1, TILE), F32),
            pltpu.VMEM((kv_count, 2 * GROUP, sent), BF16),
            pltpu.VMEM((2 * kv_count, 2 * GROUP, sent), BF16),
            pltpu.VMEM((2 * zones, 2 * GROUP, sent), BF16),
            pltpu.VMEM((2 * zones, 2 * GROUP, sent), BF16),
            pltpu.VMEM((2 * kv_count, GROUP, sent), BF16),
            pltpu.SemaphoreType.DMA((13,)),
            pltpu.SemaphoreType.DMA((10,)),
            pltpu.SemaphoreType.DMA((6 * zones + 7,)),
            pltpu.SemaphoreType.DMA((2, 2)),
        ],
        compiler_params=pltpu.CompilerParams(
            collective_id=0, has_side_effects=True, vmem_limit_bytes=48 * 1024 * 1024
        ),
    )(*[pltpu.with_memory_space_constraint(x, pltpu.HBM) for x in (
        lengths,
        tokens,
        norm_gain.reshape(1, -1),
        decay_log.reshape(1, -1),
        decay_bias.reshape(1, -1),
        head_gain.reshape(1, -1),
        mlp_gain.reshape(1, -1),
        w_alpha.T,
        w_beta.T,
        memory.reshape(memory.shape[1:]),
        w_query,
        w_key,
        w_value,
        w_outgate,
        w_output,
        w_gate,
        w_up,
        w_down,
    )])
    near = pl.BlockSpec(memory_space=pltpu.VMEM)
    out, state = pl.pallas_call(
        settle,
        out_shape=(
            jax.ShapeDtypeStruct(out.shape, out.dtype),
            jax.ShapeDtypeStruct(state.shape, state.dtype),
        ),
        in_specs=[near] * 2,
        out_specs=(far, far),
        scratch_shapes=[pltpu.SemaphoreType.DMA((2,))],
    )(*[pltpu.with_memory_space_constraint(x, pltpu.VMEM) for x in (out, state)])
    return out, state.reshape(memory.shape)


def fits(tokens, memory, w_alpha, w_gate):
    kv_count = lax.axis_size("kv")
    rows, width = tokens.shape
    live_rows = (rows // NEW) * 7 // 4
    groups = -(-live_rows // 16) * 16 // GROUP
    all_heads = w_alpha.shape[1]
    return (
        lax.axis_size("tp") == 2
        and memory.shape[0] == 1
        and memory.shape[1] == 8
        and rows == kv_count * NEW
        and rows % 16 == 0
        and width % TILE == 0
        and kv_count % groups == 0
        and w_gate.shape[1] % (kv_count // groups * TILE) == 0
        and NEW * 2 * all_heads == TILE
        and live_rows == groups * (GROUP - 1)
        and w_gate.shape[1] >= kv_count // groups * GROUP * TILE
    )


def layer(*arrays):
    if fits(arrays[0], arrays[2], arrays[8], arrays[15]):
        return fused_device(*arrays)
    return per_device(*arrays)


def solution(mesh):
    placed = (
        P(None, "kv"),
        P(),
        P("kv", "tp", None, None),
        P("kv"),
        P("kv", "tp"),
        P("kv", "tp"),
        P("kv", "tp"),
        P("kv", "tp"),
        P("kv", None),
        P("kv", None),
        P("tp"),
        P("tp"),
        P(),
        P("tp", "kv"),
        P("kv"),
        P("kv", "tp"),
        P("kv", "tp"),
        P("tp", "kv"),
    )
    return jax.shard_map(
        layer,
        mesh=mesh,
        in_specs=placed,
        out_specs=(P(None, "kv"), P("kv", "tp", None, None)),
        check_vma=False,
    )
```

```python
import jax
import jax.numpy as jnp
from jax import lax
from jax.experimental import pallas as pl
from jax.experimental.pallas import tpu as pltpu
from jax.sharding import PartitionSpec as P

D = 4096
DK = 128
DV = 128
NEW = 4


epsilon = 1e-06


def unit_rows(values):
    return values * lax.rsqrt(jnp.sum(values * values, axis=-1, keepdims=True) + epsilon)


def advance(memory, queries, key_rows, value_rows, decays, betas):
    outputs = []
    for step in range(queries.shape[1]):
        memory = jnp.exp(decays[:, step])[:, :, None, None] * memory
        predicted = jnp.einsum(
            "shde,shd->she", memory, key_rows[:, step], precision=lax.Precision.HIGHEST
        )
        correction = betas[:, step][:, :, None] * (value_rows[:, step] - predicted)
        memory = memory + key_rows[:, step][:, :, :, None] * correction[:, :, None, :]
        outputs.append(
            jnp.einsum("shde,shd->she", memory, queries[:, step], precision=lax.Precision.HIGHEST)
        )
    return (memory, jnp.stack(outputs, axis=1))


def per_device(
    tokens,
    lengths,
    memory,
    norm_gain,
    w_query,
    w_key,
    w_value,
    w_outgate,
    w_alpha,
    w_beta,
    decay_log,
    decay_bias,
    head_gain,
    w_output,
    mlp_gain,
    w_gate,
    w_up,
    w_down,
):
    total_rows = tokens.shape[0]
    kv_count = lax.axis_size("kv")
    kv_place = lax.axis_index("kv")
    tp_place = lax.axis_index("tp")
    own_rows = total_rows // kv_count
    seq_dev = memory.shape[0]
    heads_dev = memory.shape[1]
    token_f = tokens.astype(jnp.float32)
    squares = jnp.sum(token_f * token_f, axis=1)
    scaled = (token_f * norm_gain).astype(jnp.bfloat16)
    part_query = jnp.dot(scaled, w_query, preferred_element_type=jnp.float32)
    part_key = jnp.dot(scaled, w_key, preferred_element_type=jnp.float32)
    part_value = jnp.dot(scaled, w_value, preferred_element_type=jnp.float32)
    part_gate = jnp.dot(scaled, w_outgate, preferred_element_type=jnp.float32)
    part_alpha = jnp.dot(scaled, w_alpha, preferred_element_type=jnp.float32)
    part_beta = jnp.dot(scaled, w_beta, preferred_element_type=jnp.float32)
    all_squares = lax.psum(squares, "kv")
    sum_query, sum_key, sum_value, sum_gate, sum_alpha, sum_beta = (
        lax.psum_scatter(part_query, "kv", scatter_dimension=0, tiled=True),
        lax.psum_scatter(part_key, "kv", scatter_dimension=0, tiled=True),
        lax.psum_scatter(part_value, "kv", scatter_dimension=0, tiled=True),
        lax.psum_scatter(part_gate, "kv", scatter_dimension=0, tiled=True),
        lax.psum_scatter(part_alpha, "kv", scatter_dimension=0, tiled=True),
        lax.psum_scatter(part_beta, "kv", scatter_dimension=0, tiled=True),
    )
    own_squares = lax.dynamic_slice_in_dim(all_squares, kv_place * own_rows, own_rows)
    rstd = lax.rsqrt(own_squares / D + epsilon)[:, None]
    queries = (sum_query * rstd).astype(jnp.bfloat16)
    key_rows = (sum_key * rstd).astype(jnp.bfloat16)
    value_rows = (sum_value * rstd).astype(jnp.bfloat16)
    outgate = (sum_gate * rstd).astype(jnp.bfloat16)
    alphas = lax.dynamic_slice_in_dim(sum_alpha * rstd, tp_place * heads_dev, heads_dev, 1)
    beta_pre = lax.dynamic_slice_in_dim(sum_beta * rstd, tp_place * heads_dev, heads_dev, 1)
    own_lengths = lax.dynamic_slice_in_dim(lengths, kv_place * seq_dev, seq_dev)
    live = jnp.arange(NEW, dtype=jnp.int32)[None, :] < own_lengths[:, None]
    query_h = unit_rows(queries.astype(jnp.float32).reshape(seq_dev, NEW, heads_dev, DK)) * DK ** (
        -0.5
    )
    key_h = unit_rows(key_rows.astype(jnp.float32).reshape(seq_dev, NEW, heads_dev, DK))
    value_h = value_rows.astype(jnp.float32).reshape(seq_dev, NEW, heads_dev, DV)
    decays = -jnp.exp(decay_log) * jax.nn.softplus(alphas + decay_bias)
    decays = jnp.where(live[:, :, None], decays.reshape(seq_dev, NEW, heads_dev), 0.0)
    betas = jnp.where(
        live[:, :, None], jax.nn.sigmoid(beta_pre).reshape(seq_dev, NEW, heads_dev), 0.0
    )
    new_memory, attended = advance(memory, query_h, key_h, value_h, decays, betas)
    attended = attended * lax.rsqrt(jnp.mean(attended * attended, axis=-1, keepdims=True) + epsilon)
    gate_h = outgate.astype(jnp.float32).reshape(seq_dev, NEW, heads_dev, DV)
    mixed = (
        (attended * head_gain * jax.nn.silu(gate_h))
        .astype(jnp.bfloat16)
        .reshape(own_rows, heads_dev * DV)
    )
    attn_terms = jnp.dot(
        lax.all_gather(mixed, "kv", axis=0, tiled=True),
        w_output,
        preferred_element_type=jnp.float32,
    )
    attn_total = lax.psum(attn_terms, "tp")
    hidden = (token_f + attn_total).astype(jnp.bfloat16)
    hidden_f = hidden.astype(jnp.float32)
    hidden_squares = jnp.sum(hidden_f * hidden_f, axis=1)
    hscaled = (hidden_f * mlp_gain).astype(jnp.bfloat16)
    all_live = (jnp.arange(NEW, dtype=jnp.int32)[None, :] < lengths[:, None]).reshape(total_rows)
    part_gate_rows = jnp.dot(hscaled, w_gate, preferred_element_type=jnp.float32)
    part_up_rows = jnp.dot(hscaled, w_up, preferred_element_type=jnp.float32)
    gate_rows, up_rows, mlp_squares = lax.psum((part_gate_rows, part_up_rows, hidden_squares), "kv")
    rstd2 = lax.rsqrt(mlp_squares / D + epsilon)[:, None]
    active = (jax.nn.silu(gate_rows * rstd2) * (up_rows * rstd2)).astype(jnp.bfloat16)
    feed_terms = jnp.dot(active, w_down, preferred_element_type=jnp.float32)
    feed_total = lax.psum(feed_terms.astype(jnp.bfloat16), "tp").astype(jnp.float32)
    layer_out = jnp.where(all_live[:, None], hidden_f + feed_total, 0.0).astype(jnp.bfloat16)
    return (layer_out, new_memory)


F32 = jnp.float32
BF16 = jnp.bfloat16
HIGH = lax.Precision.HIGHEST
TILE = 128
GROUP = 8


def iota(shape, axis):
    return lax.broadcasted_iota(jnp.int32, shape, axis)


def dot(a, b, precision=None):
    return jnp.dot(a, b, preferred_element_type=F32, precision=precision)


def fused(
    lens_far,
    tokens_far,
    norm_far,
    decay_log_far,
    decay_bias_far,
    head_far,
    mlp_far,
    alpha_far,
    beta_far,
    memory,
    w_query,
    w_key,
    w_value,
    w_outgate,
    w_output,
    w_gate,
    w_up,
    w_down,
    out,
    v_mem,
    lens,
    tokens,
    norm_gain,
    decay_in,
    head_gain,
    mlp_gain,
    v_ab,
    v_proj,
    v_output,
    v_gu,
    v_down,
    proj_send,
    proj_recv,
    proj_part,
    proj_last,
    pf_recv,
    pf_part,
    pf_last,
    small_send,
    small_recv,
    small_part,
    small_last,
    rs_buf,
    xs_buf,
    kq_buf,
    r_buf,
    u_buf,
    a_buf,
    mix_buf,
    mix_all,
    tp_send,
    tp_recv,
    sq_send,
    sq_recv,
    gu_send,
    gu_recv,
    gu_part,
    gu_last,
    zf_recv,
    zf_part,
    zf_last,
    act_all,
    load_sem,
    send_sem,
    recv_sem,
    tp_sem,
):
    kv_count = mix_all.shape[0]
    me = lax.axis_index("kv")
    tp = lax.axis_index("tp")
    rows, width = tokens.shape
    heads = v_mem.shape[0]
    wide = heads * DV
    compact = tp_send.shape[1]
    groups = compact // GROUP
    zones = kv_count // groups
    sent = gu_send.shape[2]
    chunk = sent + TILE
    held = GROUP - 1
    main = gu_recv.shape[2]
    wide_main = proj_recv.shape[2]
    total_width = width * kv_count
    all_heads = v_ab.shape[1]
    zone_me = me // groups
    group_me = lax.rem(me, groups)
    steps = [*range(1, zones), 0]
    side, odd = zone_me // 2, lax.rem(zone_me, 2)

    def zone_of(step):
        if zones != 4:
            return lax.rem(zone_me + step, zones)
        end = 1 - (side - odd) * (side - odd)
        far_end, near_end = (1 - side) * 3, side * 3
        far_mid, near_mid = 2 - side, 1 + side
        second = end * far_mid + (1 - end) * near_end
        third = end * near_mid + (1 - end) * far_mid
        return [zone_me, far_end, second, third][step]

    def peer(g):
        if groups != 4:
            return lax.rem(group_me + g, groups)
        row, col = group_me // 2, lax.rem(group_me, 2)
        return [
            group_me,
            (1 - row) * 2 + 1 - col,
            row * 2 + 1 - col,
            (1 - row) * 2 + col,
        ][g]

    barrier = pltpu.get_barrier_semaphore()

    def greet(**where):
        pl.semaphore_signal(
            barrier, inc=1, device_id=where, device_id_type=pl.DeviceIdType.MESH
        )

    for core in (tp, 1 - tp):
        for g in range(1, groups):
            greet(kv=zone_me * groups + peer(g), tp=core)
        for step in steps[:-1]:
            greet(kv=zone_of(step) * groups + group_me, tp=core)
    greet(tp=1 - tp)

    def load(src, dst, sem):
        return pltpu.make_async_copy(src, dst, load_sem.at[sem])

    half = wide // 2
    halves = [slice(c * half, (c + 1) * half) for c in range(2)]
    load(tokens_far, tokens, 0).start()
    load(norm_far, norm_gain, 1).start()
    load(alpha_far, v_ab.at[0], 2).start()
    load(beta_far, v_ab.at[1], 2).start()
    for c in (1, 0):
        for p, weight in enumerate((w_query, w_key, w_value, w_outgate)):
            load(weight.at[:, halves[c]], v_proj.at[p, :, halves[c]], 3 + c).start()
    load(lens_far, lens, 5).start()
    load(decay_log_far, decay_in.at[0], 6).start()
    load(decay_bias_far, decay_in.at[1], 6).start()
    load(head_far, head_gain, 7).start()
    load(mlp_far, mlp_gain, 8).start()

    def loaded(ref, sem):
        load(ref, ref, sem).wait()

    plane_sem, gu_sem, near_sem, far_sem = 0, zones, 3 * zones, 5 * zones
    proj_sem, mlp_sem, mix_sem, small_sem, few_sem, sq_sem = range(6 * zones, 6 * zones + 6)
    both_sem = 6 * zones + 6
    first_sem, then_sem = 6 * zones + 7, 6 * zones + 9
    early_sem, onward_sem = 6 * zones + 11, 6 * zones + 12

    def remote(src, dst, sent, arrival, partner, core=None):
        return pltpu.make_async_remote_copy(
            src_ref=src,
            dst_ref=dst,
            send_sem=send_sem.at[sent],
            recv_sem=recv_sem.at[arrival],
            device_id={"kv": partner, "tp": tp if core is None else core},
            device_id_type=pl.DeviceIdType.MESH,
        )

    def arrived(ref, arrival):
        remote(ref, ref, 0, arrival, me).wait_recv()

    def left(ref, sent):
        remote(ref, ref, sent, 0, me).wait_send()

    def tp_swap(phase, value, meanwhile=None):
        tp_send[phase] = value
        swap = pltpu.make_async_remote_copy(
            src_ref=tp_send.at[phase],
            dst_ref=tp_recv.at[phase],
            send_sem=tp_sem.at[phase, 0],
            recv_sem=tp_sem.at[phase, 1],
            device_id={"tp": 1 - tp},
            device_id_type=pl.DeviceIdType.MESH,
        )
        swap.start()
        if meanwhile is not None:
            meanwhile()
        swap.wait()
        return value + tp_recv[phase]

    packed_rows = kv_count * 2 * NEW
    row = iota((packed_rows, rows), 0)
    spread = jnp.where(
        iota((packed_rows, rows), 1) == (row >> 3) * NEW + (row & 3), 1.0, 0.0
    ).astype(BF16)
    seq_row = iota((kv_count, rows), 0)
    seq_row = lax.rem(seq_row, zones) * groups + seq_row // zones
    lane = iota((kv_count, TILE), 1)
    place = iota((TILE, all_heads), 0) & (2 * all_heads - 1)
    head_of = iota((TILE, all_heads), 1)
    one_alpha = jnp.where(place == head_of, 1.0, 0.0).astype(BF16)
    one_beta = jnp.where(place == head_of + all_heads, 1.0, 0.0).astype(BF16)
    loaded(tokens, 0)
    loaded(norm_gain, 1)
    tok = tokens[...]
    scaled = (tok.astype(F32) * norm_gain[...]).astype(BF16)
    wide_scaled = dot(spread, scaled)
    part_of = iota((packed_rows, width), 0) & 7
    low = jnp.where(part_of < NEW, wide_scaled, 0.0).astype(BF16)
    high = jnp.where(part_of >= NEW, wide_scaled, 0.0).astype(BF16)

    def sum_plane(recv, sem, first, own):
        count = groups if own is None else groups - 1
        arrived(recv.at[pl.ds(first, count)], sem)
        added = (recv[first + group_me] if own is None else own).astype(F32)
        for g in range(1, groups):
            added = added + recv[first + peer(g)].astype(F32)
        return added

    def send_proj(zone, cols=slice(0, wide_main)):
        def send(slab, place, partner):
            remote(
                proj_send.at[slab, :, cols],
                proj_recv.at[place, :, cols],
                1,
                plane_sem + zone,
                partner,
                1 - tp,
            ).start()

        for g in range(1, groups):
            send(
                zone * groups + peer(g),
                zone * groups + group_me,
                zone_me * groups + peer(g),
            )
        send(zone * groups + group_me, zone * groups + group_me, me)

    for c in (1, 0):
        loaded(v_proj.at[:, :, halves[c]], 3 + c)
        parts = [
            dot(low, v_proj[p, :, halves[c]]) + dot(high, v_proj[p + 1, :, halves[c]])
            for p in (0, 2)
        ]
        parts = [part.reshape(kv_count, 2 * NEW, half) for part in parts]
        proj_send[:, :, halves[c]] = jnp.concatenate(parts, axis=1).astype(BF16)
        if c:
            pl.semaphore_wait(barrier, 2 * (groups + zones - 2) + 1)
            for step in steps:
                zone = zone_of(step)
                remote(
                    proj_send.at[pl.ds(zone * groups, groups), :, wide_main:],
                    pf_recv.at[zone_me],
                    12,
                    early_sem,
                    zone * groups + group_me,
                    1 - tp,
                ).start()
        send_proj(zone_of(steps[0]), slice(c * half, wide_main if c else half))
    load(memory, v_mem, 9).start()
    load(w_output, v_output, 10).start()
    load(w_gate, v_gu.at[0], 11).start()
    load(w_up, v_gu.at[1], 11).start()
    load(w_down, v_down, 12).start()
    loaded(v_ab, 2)
    w_small = (dot(one_alpha, v_ab[0]) + dot(one_beta, v_ab[1])).astype(BF16)
    small = jnp.zeros((kv_count, TILE), F32)
    squares = jnp.zeros((kv_count, TILE), F32)
    for t in range(NEW):
        take = jnp.where(iota((kv_count, rows), 1) == seq_row * NEW + t, 1.0, 0.0).astype(BF16)
        took = lax.dot_general(
            dot(take, scaled).astype(BF16),
            w_small,
            (((1,), (1,)), ((), ())),
            preferred_element_type=F32,
        )
        small = jnp.where(lane // (2 * all_heads) == t, took, small)
        tok_t = dot(take, tok)
        squares = jnp.where(
            lane == t, jnp.sum(tok_t * tok_t, axis=1, keepdims=True), squares
        )
    small_send[:, :, 0, :] = small.reshape(groups, zones, TILE)
    small_send[:, :, 1, :] = squares.reshape(groups, zones, TILE)
    for g in range(1, groups):
        remote(
            small_send.at[peer(g)],
            small_recv.at[group_me],
            0,
            small_sem,
            zone_me * groups + peer(g),
        ).start()
    for step in steps[1:-1]:
        send_proj(zone_of(step))
    for g in range(1, groups):
        remote(
            proj_send.at[zone_me * groups + peer(g), :, :wide_main],
            proj_recv.at[me],
            1,
            plane_sem + zone_me,
            zone_me * groups + peer(g),
        ).start()

    loaded(lens, 5)
    loaded(decay_in, 6)
    loaded(head_gain, 7)
    loaded(mlp_gain, 8)
    slots_wide = kv_count * heads * NEW
    shape_a = (1, rows)
    shape_b = (1, slots_wide)
    shape_c = (rows, compact)
    length_a = jnp.zeros(shape_a, jnp.int32)
    start_a = jnp.zeros(shape_a, jnp.int32)
    length_b = jnp.zeros(shape_b, jnp.int32)
    start_b = jnp.zeros(shape_b, jnp.int32)
    length_c = jnp.zeros(shape_c, jnp.int32)
    start_c = jnp.zeros(shape_c, jnp.int32)
    seq_a = iota(shape_a, 1) >> 2
    seq_b = iota(shape_b, 1) >> 5
    seq_c = iota(shape_c, 0) >> 2
    begin = jnp.int32(0)
    for s in range(kv_count):
        length_a = jnp.where(seq_a == s, lens[s], length_a)
        start_a = jnp.where(seq_a == s, begin, start_a)
        length_b = jnp.where(seq_b == s, lens[s], length_b)
        start_b = jnp.where(seq_b == s, begin, start_b)
        length_c = jnp.where(seq_c == s, lens[s], length_c)
        start_c = jnp.where(seq_c == s, begin, start_c)
        begin = begin + lens[s]
    slot_a = iota(shape_a, 1) & 3

    def padded(rank):
        return sum(((rank >= g * held).astype(jnp.int32) for g in range(1, groups)), rank)

    rank_a = jnp.where(slot_a < length_a, padded(start_a + slot_a), -1)
    pack = jnp.where(rank_a == iota((compact, rows), 0), 1.0, 0.0).astype(BF16)
    slot_c = iota(shape_c, 0) & 3
    rank_c = jnp.where(slot_c < length_c, padded(start_c + slot_c), -1)
    unpack = jnp.where(rank_c == iota(shape_c, 1), 1.0, 0.0).astype(BF16)
    slot_b = iota(shape_b, 1) & 3
    head_b = (iota(shape_b, 1) >> 2) & (heads - 1)
    rank_b = jnp.where(slot_b < length_b, head_b * compact + padded(start_b + slot_b), -1)
    collect = jnp.where(rank_b == iota((heads * compact, slots_wide), 0), 1.0, 0.0).astype(BF16)
    tok_packed = dot(pack, tok)

    def proj_onward(zone):
        proj_part[zone] = sum_plane(proj_recv, plane_sem + zone, zone * groups, None).astype(BF16)
        remote(
            proj_part.at[zone],
            proj_last.at[zone_me],
            3,
            proj_sem,
            zone * groups + group_me,
            1 - tp,
        ).start()

    proj_onward(zone_of(steps[0]))
    arrived(small_recv.at[pl.ds(0, groups - 1)], small_sem)
    small = small_send[group_me]
    for g in range(1, groups):
        small = small + small_recv[peer(g)]
    small_part[...] = small
    for step in steps[:-1]:
        zone = zone_of(step)
        remote(
            small_part.at[zone], small_last.at[zone_me], 2, few_sem, zone * groups + group_me
        ).start()

    proj_onward(zone_of(steps[1]))
    arrived(pf_recv, early_sem)
    early = pf_recv[0].astype(F32)
    for zone in range(1, zones):
        early = early + pf_recv[zone].astype(F32)
    pf_part[...] = early.astype(BF16)
    for g in [*range(1, groups), 0]:
        remote(
            pf_part.at[peer(g)],
            pf_last.at[group_me],
            13,
            onward_sem,
            zone_me * groups + peer(g),
            1 - tp,
        ).start()
    for step in steps[2:-1]:
        proj_onward(zone_of(step))
    total = sum_plane(proj_recv, plane_sem + zone_me, zone_me * groups, proj_send[me, :, :wide_main])
    arrived(small_last.at[pl.ds(0, zones - 1)], few_sem)
    small = small_part[zone_me]
    for step in steps[:-1]:
        small = small + small_last[zone_of(step)]
    diagonal = iota((NEW, TILE), 0) == iota((NEW, TILE), 1)
    mean_sq = jnp.sum(jnp.where(diagonal, small[1:2, :], 0.0), axis=1, keepdims=True)
    rstd = lax.rsqrt(mean_sq / total_width + epsilon)
    rstd_wide = jnp.broadcast_to(rstd, (NEW, TILE))
    for p in range(4):
        rs_buf[p * NEW : (p + 1) * NEW, :] = rstd_wide
    eye = iota((heads, heads), 0) == iota((heads, heads), 1)
    rate = jnp.sum(jnp.where(eye, jnp.exp(decay_in[0]), 0.0), axis=1, keepdims=True)
    bias = jnp.sum(jnp.where(eye, decay_in[1], 0.0), axis=1, keepdims=True)
    pick = iota((heads, TILE), 1) - iota((heads, TILE), 0) - tp * heads
    own_length = jnp.full((heads, 1), lens[me], jnp.int32)
    decay, beta = [], []
    for t in range(NEW):
        line = small[0:1, :]
        first = 2 * all_heads * t
        scale_t = rstd[t : t + 1, :]
        alpha = jnp.sum(jnp.where(pick == first, line, 0.0), axis=1, keepdims=True) * scale_t
        write = (
            jnp.sum(jnp.where(pick == first + all_heads, line, 0.0), axis=1, keepdims=True)
            * scale_t
        )
        x = alpha + bias
        soft = jnp.maximum(x, 0.0) + jnp.log1p(jnp.exp(-jnp.abs(x)))
        live = own_length > t
        decay.append(jnp.exp(jnp.where(live, -rate * soft, 0.0)))
        beta.append(jnp.where(live, jax.nn.sigmoid(write), 0.0))
    loaded(v_mem, 9)
    arrived(proj_last.at[pl.ds(0, zones - 1)], proj_sem)
    for step in steps[:-1]:
        total = total + proj_last[zone_of(step)].astype(F32)
    arrived(pf_last, onward_sem)
    early = pf_last[0].astype(F32)
    for g in range(1, groups):
        early = early + pf_last[g].astype(F32)
    total = jnp.concatenate([total, early], axis=1)
    scale = rs_buf[...]
    for h in range(heads):
        piece = total[:, h * DV : (h + 1) * DV] * scale
        xs_buf[h * 16 : (h + 1) * 16, :] = piece.astype(BF16).astype(F32)

    def slot_rows(ref, index, stride):
        return ref[pl.ds(index, heads, stride=stride), :]

    query, key_rows, value, gate = (
        [slot_rows(xs_buf, p * NEW + t, 16) for t in range(NEW)] for p in range(4)
    )
    query = [unit_rows(x) * DK ** (-0.5) for x in query]
    key_rows = [unit_rows(x) for x in key_rows]
    for t in range(NEW):
        kq_buf[pl.ds(t, heads, stride=8), :] = key_rows[t]
        kq_buf[pl.ds(NEW + t, heads, stride=8), :] = query[t]
    for h in range(heads):
        r_buf[h * 8 : (h + 1) * 8, :] = dot(kq_buf[h * 8 : (h + 1) * 8, :], v_mem[h], HIGH)
    seen_k = [slot_rows(r_buf, t, 8) for t in range(NEW)]
    seen_q = [slot_rows(r_buf, NEW + t, 8) for t in range(NEW)]

    def inner(a, b):
        return jnp.sum(a * b, axis=1, keepdims=True)

    corrections = []
    for t in range(NEW):
        for r in range(t, NEW):
            seen_k[r] = seen_k[r] * decay[t]
            seen_q[r] = seen_q[r] * decay[t]
        fix = beta[t] * (value[t] - seen_k[t])
        corrections.append(fix)
        for r in range(t, NEW):
            if r > t:
                seen_k[r] = seen_k[r] + inner(key_rows[t], key_rows[r]) * fix
            seen_q[r] = seen_q[r] + inner(key_rows[t], query[r]) * fix
    for t in range(NEW):
        o = seen_q[t]
        o = o * lax.rsqrt(jnp.mean(o * o, axis=1, keepdims=True) + epsilon)
        o = o * head_gain[...] * (gate[t] * jax.nn.sigmoid(gate[t]))
        mix_buf[pl.ds(t, heads, stride=NEW), :] = o
    mix_all[me] = mix_buf[...].astype(BF16)

    def send_mix():
        for step in steps:
            for g in [*range(1, groups), 0]:
                if step or g:
                    to = zone_of(step) * groups + peer(g)
                    remote(mix_all.at[me], mix_all.at[me], 4, mix_sem, to).start()

    send_mix()
    u_buf[...] = jnp.zeros_like(u_buf)
    after = jnp.ones((heads, 1), F32)
    for t in range(NEW - 1, -1, -1):
        u_buf[pl.ds(t, heads, stride=8), :] = corrections[t] * after
        after = after * decay[t]
    a_buf[...] = jnp.broadcast_to(after, (heads, TILE))
    for h in range(heads):
        outer = lax.dot_general(
            kq_buf[h * 8 : (h + 1) * 8, :],
            u_buf[h * 8 : (h + 1) * 8, :],
            (((0,), (0,)), ((), ())),
            precision=HIGH,
            preferred_element_type=F32,
        )
        v_mem[h] = v_mem[h] * a_buf[h : h + 1, :] + outer
    loaded(v_output, 10)
    loaded(v_gu, 11)
    loaded(v_down, 12)

    arrived(mix_all.at[pl.ds(0, kv_count - 1)], mix_sem)
    gathered = mix_all[...].reshape(slots_wide, DV)
    packed = dot(collect, gathered).astype(BF16)
    packed = jnp.concatenate(
        [packed[h * compact : (h + 1) * compact, :] for h in range(heads)], axis=1
    )
    attended = tp_swap(0, dot(packed, v_output[...]))
    hidden = (tok_packed + attended).astype(BF16).astype(F32)

    hscaled = hidden * mlp_gain[...]
    blank = jnp.zeros((GROUP, width), F32)
    gate_rows = []
    for g in range(groups):
        gate_rows += [hscaled[g * GROUP : (g + 1) * GROUP, :], blank]
    gate_rows = jnp.concatenate(gate_rows, axis=0)
    up_rows = pltpu.roll(gate_rows, held, 0).astype(BF16)
    gate_rows = gate_rows.astype(BF16)
    spare = (iota((2 * compact, TILE), 0) & (2 * GROUP - 1)) >= 2 * held
    for step in steps:
        zone = zone_of(step)
        cols = pl.ds(pl.multiple_of(zone * chunk, TILE), chunk)
        term = dot(gate_rows, v_gu[0, :, cols]) + dot(up_rows, v_gu[1, :, cols])
        last = term[:, sent:]
        tiles = [
            jnp.where(
                spare,
                pltpu.roll(last, 2 * (held - k), 0),
                term[:, k * TILE : (k + 1) * TILE],
            )
            for k in range(held)
        ]
        term = jnp.concatenate([*tiles, term[:, held * TILE : sent]], axis=1)
        gu_send[pl.ds(zone * groups, groups)] = term.astype(BF16).reshape(
            groups, 2 * GROUP, sent
        )
        arrival = gu_sem + tp * zones + zone
        for g in range(1, groups):
            remote(
                gu_send.at[zone * groups + peer(g), :, :main],
                gu_recv.at[tp * kv_count + zone * groups + group_me],
                6,
                arrival,
                zone_me * groups + peer(g),
                1,
            ).start()

        rest = gu_send.at[pl.ds(zone * groups, groups), :, main:]
        lands = zf_recv.at[tp * zones + zone_me]
        if step:
            there = zone * groups + group_me
            remote(rest, lands, 10, first_sem + tp, there, 1).start()

        @pl.when(tp == 0)
        def _():
            slab = zone * groups + group_me
            remote(gu_send.at[slab, :, :main], gu_recv.at[slab], 6, arrival, me, 1).start()
            if not step:
                remote(rest, lands, 10, first_sem, me, 1).start()

        if step == steps[0]:

            @pl.when(tp == 1)
            def _():
                squares = jnp.sum(hidden * hidden, axis=1, keepdims=True)
                spot = (iota((compact, TILE), 0) & (GROUP - 1)) == iota((compact, TILE), 1)
                squares = jnp.sum(jnp.where(spot, squares, 0.0).reshape(groups, GROUP, TILE), axis=1)
                sq_send[...] = squares.reshape(groups, 1, TILE)
                sq_recv[me] = sq_send[group_me]

                @pl.loop(1, kv_count)
                def _(off):
                    to = lax.rem(me + off, kv_count)
                    remote(sq_send.at[lax.rem(to, groups)], sq_recv.at[me], 5, sq_sem, to).start()

    near_first = steps[::-1]

    @pl.when(tp == 1)
    def _():
        def plane_total(zone, core):
            slab = zone * groups
            own = gu_send[slab + group_me, :, :main] if core else None
            return sum_plane(gu_recv, gu_sem + core * zones + zone, core * kv_count + slab, own)

        def zones_total(core):
            arrived(zf_recv.at[pl.ds(core * zones, zones - core)], first_sem + core)
            if core:
                added = gu_send[pl.ds(zone_me * groups, groups), :, main:].astype(F32)
            else:
                added = zf_recv[zone_me].astype(F32)
            for step in steps[:-1]:
                added = added + zf_recv[core * zones + zone_of(step)].astype(F32)
            zf_part[pl.ds(core * groups, groups)] = added.astype(BF16)
            for g in range(1, groups):
                remote(
                    zf_part.at[core * groups + peer(g)],
                    zf_last.at[core * groups + group_me],
                    11,
                    then_sem + core,
                    zone_me * groups + peer(g),
                ).start()

        for step in steps[:-1]:
            zone = zone_of(step)
            for core in (1, 0):
                gu_part[core * zones + zone] = plane_total(zone, core).astype(BF16)
                remote(
                    gu_part.at[core * zones + zone],
                    gu_last.at[core * zones + zone_me],
                    7,
                    mlp_sem if core else both_sem,
                    zone * groups + group_me,
                ).start()
            if step == steps[1]:
                for core in (1, 0):
                    zones_total(core)
        arrived(sq_recv.at[pl.ds(0, kv_count - 1)], sq_sem)
        mean_sq = jnp.sum(sq_recv[...].reshape(kv_count, TILE), axis=0, keepdims=True)
        spot = iota((GROUP, TILE), 0) == iota((GROUP, TILE), 1)
        mean_sq = jnp.sum(jnp.where(spot, mean_sq, 0.0), axis=1, keepdims=True)
        rstd2 = lax.rsqrt(mean_sq / total_width + epsilon)

        def pass_on(zone, core, sent, arrival, partner, there):
            block = core * kv_count + zone * groups + group_me
            remote(act_all.at[block], act_all.at[block], sent, arrival, partner, there).start()

        def forward(zone, core):
            for g in range(1, groups):
                pass_on(zone, core, 9, far_sem + zone, zone_me * groups + peer(g), core)
            if core == 0:
                pass_on(zone, 0, 9, far_sem + zone, me, 0)

        for core in (0, 1):
            both = plane_total(zone_me, core)
            arrived(
                gu_last.at[pl.ds(core * zones, zones - 1)], mlp_sem if core else both_sem
            )
            for step in steps[:-1]:
                both = both + gu_last[core * zones + zone_of(step)].astype(F32)
            arrived(zf_last.at[pl.ds(core * groups, groups - 1)], then_sem + core)
            apart = zf_part[core * groups + group_me].astype(F32)
            for g in range(1, groups):
                apart = apart + zf_last[core * groups + peer(g)].astype(F32)
            both = jnp.concatenate([both, apart], axis=1)
            row = iota((2 * GROUP, TILE), 0)
            last = jnp.zeros((2 * GROUP, TILE), F32)
            for k in range(held):
                tile = both[:, k * TILE : (k + 1) * TILE]
                back = pltpu.roll(tile, 2 * GROUP - 2 * (held - k), 0)
                last = jnp.where(row >> 1 == k, back, last)
            both = jnp.concatenate([both, last], axis=1)
            gated = both[:GROUP] * rstd2
            lifted = pltpu.roll(both, 2 * GROUP - held, 0)[:GROUP] * rstd2
            active = gated * jax.nn.sigmoid(gated) * lifted
            row = iota((GROUP, TILE), 0)
            last = active[:, sent:]
            tiles = [
                jnp.where(
                    row == held,
                    last if k == held else pltpu.roll(last, held - k, 0),
                    active[:, k * TILE : (k + 1) * TILE],
                )
                for k in range(held)
            ]
            active = jnp.concatenate([*tiles, active[:, held * TILE : sent]], axis=1)
            act_all[core * kv_count + me] = active.astype(BF16)
            for step in steps[:-1]:
                there = zone_of(step) * groups + group_me
                pass_on(zone_me, core, 8, near_sem + core * zones + zone_me, there, 1)
            forward(zone_me, core)
        for step in near_first[1:]:
            zone = zone_of(step)
            for core in (0, 1):
                block = core * kv_count + zone * groups + group_me
                arrived(act_all.at[block], near_sem + core * zones + zone)
                forward(zone, core)

    feed = jnp.zeros((compact, width), F32)
    row_in = iota((compact, TILE), 0) & (GROUP - 1)
    for step in near_first:
        zone = zone_of(step)
        first = tp * kv_count + zone * groups

        @pl.when(tp == 0)
        def _():
            arrived(act_all.at[pl.ds(first, groups)], far_sem + zone)

        @pl.when(tp == 1)
        def _():
            arrived(act_all.at[pl.ds(first, groups - 1)], far_sem + zone)

        part = act_all[pl.ds(first, groups)].astype(F32).reshape(compact, sent)
        last = jnp.zeros((compact, TILE), F32)
        for k in range(held):
            tile = part[:, k * TILE : (k + 1) * TILE]
            last = jnp.where(row_in == k, pltpu.roll(tile, compact - (held - k), 0), last)
        part = jnp.concatenate([part, last], axis=1)
        cols = pl.ds(pl.multiple_of(zone * chunk, TILE), chunk)
        feed = feed + dot(part.astype(BF16), v_down[cols, :])

    def drain():
        left(small_send.at[pl.ds(0, groups - 1)], 0)
        left(proj_recv.at[pl.ds(0, kv_count - 1)], 1)
        left(pf_recv, 12)
        left(pf_last, 13)
        left(small_part.at[pl.ds(0, zones - 1)], 2)
        left(proj_part.at[pl.ds(0, zones - 1)], 3)
        left(mix_all.at[pl.ds(0, kv_count - 1)], 4)

        @pl.when(tp == 0)
        def _():
            left(gu_recv.at[pl.ds(0, kv_count)], 6)
            left(zf_recv.at[pl.ds(0, zones)], 10)

        @pl.when(tp == 1)
        def _():
            left(sq_recv.at[pl.ds(0, kv_count - 1)], 5)
            left(gu_recv.at[pl.ds(0, kv_count - zones)], 6)
            left(zf_recv.at[pl.ds(0, zones - 1)], 10)
            left(zf_last.at[pl.ds(0, 2 * (groups - 1))], 11)
            left(gu_part.at[pl.ds(0, 2 * (zones - 1))], 7)
            left(act_all.at[pl.ds(0, 2 * (zones - 1))], 8)
            left(act_all.at[pl.ds(0, zones * (2 * groups - 1))], 9)

    result = hidden + tp_swap(1, feed, drain)
    result = jnp.where((iota((compact, width), 0) & (GROUP - 1)) < held, result, 0.0)
    result = result.astype(BF16)
    out[...] = dot(unpack, result).astype(BF16)


def settle(out, state, out_far, state_far, sem):
    moves = [
        pltpu.make_async_copy(state, state_far, sem.at[0]),
        pltpu.make_async_copy(out, out_far, sem.at[1]),
    ]
    for move in moves:
        move.start()
    for move in moves:
        move.wait()


def fused_device(
    tokens,
    lengths,
    memory,
    norm_gain,
    w_query,
    w_key,
    w_value,
    w_outgate,
    w_alpha,
    w_beta,
    decay_log,
    decay_bias,
    head_gain,
    w_output,
    mlp_gain,
    w_gate,
    w_up,
    w_down,
):
    kv_count = lax.axis_size("kv")
    rows, width = tokens.shape
    heads = memory.shape[1]
    all_heads = w_alpha.shape[1]
    live_rows = (rows // NEW) * 7 // 4
    compact = -(-live_rows // 16) * 16
    groups = compact // GROUP
    zones = kv_count // groups
    sent = w_gate.shape[1] // zones - TILE
    main = sent - 2 * TILE
    wide = heads * DV
    early = 2 * TILE
    near = pl.BlockSpec(memory_space=pltpu.VMEM)
    far = pl.BlockSpec(memory_space=pltpu.HBM)
    out, state = pl.pallas_call(
        fused,
        out_shape=(
            jax.ShapeDtypeStruct((rows, width), BF16),
            jax.ShapeDtypeStruct(memory.shape[1:], F32),
        ),
        in_specs=[far] * 18,
        out_specs=(near, near),
        scratch_shapes=[
            pltpu.SMEM(lengths.shape, jnp.int32),
            pltpu.VMEM((rows, width), BF16),
            pltpu.VMEM((1, width), F32),
            pltpu.VMEM((2, 1, heads), F32),
            pltpu.VMEM((1, DV), F32),
            pltpu.VMEM((1, width), F32),
            pltpu.VMEM((2, all_heads, width), BF16),
            pltpu.VMEM((4, *w_query.shape), BF16),
            pltpu.VMEM(w_output.shape, BF16),
            pltpu.VMEM((2, *w_gate.shape), BF16),
            pltpu.VMEM(w_down.shape, BF16),
            pltpu.VMEM((kv_count, 16, wide), BF16),
            pltpu.VMEM((kv_count, 16, wide - early), BF16),
            pltpu.VMEM((zones, 16, wide - early), BF16),
            pltpu.VMEM((zones, 16, wide - early), BF16),
            pltpu.VMEM((zones, groups, 16, early), BF16),
            pltpu.VMEM((groups, 16, early), BF16),
            pltpu.VMEM((groups, 16, early), BF16),
            pltpu.VMEM((groups, zones, 2, TILE), F32),
            pltpu.VMEM((groups, zones, 2, TILE), F32),
            pltpu.VMEM((zones, 2, TILE), F32),
            pltpu.VMEM((zones, 2, TILE), F32),
            pltpu.VMEM((16, TILE), F32),
            pltpu.VMEM((heads * 16, TILE), F32),
            pltpu.VMEM((heads * 8, TILE), F32),
            pltpu.VMEM((heads * 8, TILE), F32),
            pltpu.VMEM((heads * 8, TILE), F32),
            pltpu.VMEM((heads, TILE), F32),
            pltpu.VMEM((heads * NEW, TILE), F32),
            pltpu.VMEM((kv_count, heads * NEW, TILE), BF16),
            pltpu.VMEM((2, compact, width), F32),
            pltpu.VMEM((2, compact, width), F32),
            pltpu.VMEM((groups, 1, TILE), F32),
            pltpu.VMEM((kv_count, 1, TILE), F32),
            pltpu.VMEM((kv_count, 2 * GROUP, sent), BF16),
            pltpu.VMEM((2 * kv_count, 2 * GROUP, main), BF16),
            pltpu.VMEM((2 * zones, 2 * GROUP, main), BF16),
            pltpu.VMEM((2 * zones, 2 * GROUP, main), BF16),
            pltpu.VMEM((2 * zones, groups, 2 * GROUP, sent - main), BF16),
            pltpu.VMEM((2 * groups, 2 * GROUP, sent - main), BF16),
            pltpu.VMEM((2 * groups, 2 * GROUP, sent - main), BF16),
            pltpu.VMEM((2 * kv_count, GROUP, sent), BF16),
            pltpu.SemaphoreType.DMA((13,)),
            pltpu.SemaphoreType.DMA((14,)),
            pltpu.SemaphoreType.DMA((6 * zones + 13,)),
            pltpu.SemaphoreType.DMA((2, 2)),
        ],
        compiler_params=pltpu.CompilerParams(
            collective_id=0, has_side_effects=True, vmem_limit_bytes=48 * 1024 * 1024
        ),
    )(*[pltpu.with_memory_space_constraint(x, pltpu.HBM) for x in (
        lengths,
        tokens,
        norm_gain.reshape(1, -1),
        decay_log.reshape(1, -1),
        decay_bias.reshape(1, -1),
        head_gain.reshape(1, -1),
        mlp_gain.reshape(1, -1),
        w_alpha.T,
        w_beta.T,
        memory.reshape(memory.shape[1:]),
        w_query,
        w_key,
        w_value,
        w_outgate,
        w_output,
        w_gate,
        w_up,
        w_down,
    )])
    near = pl.BlockSpec(memory_space=pltpu.VMEM)
    out, state = pl.pallas_call(
        settle,
        out_shape=(
            jax.ShapeDtypeStruct(out.shape, out.dtype),
            jax.ShapeDtypeStruct(state.shape, state.dtype),
        ),
        in_specs=[near] * 2,
        out_specs=(far, far),
        scratch_shapes=[pltpu.SemaphoreType.DMA((2,))],
    )(*[pltpu.with_memory_space_constraint(x, pltpu.VMEM) for x in (out, state)])
    return out, state.reshape(memory.shape)


def fits(tokens, memory, w_alpha, w_gate):
    kv_count = lax.axis_size("kv")
    rows, width = tokens.shape
    live_rows = (rows // NEW) * 7 // 4
    groups = -(-live_rows // 16) * 16 // GROUP
    all_heads = w_alpha.shape[1]
    return (
        lax.axis_size("tp") == 2
        and memory.shape[0] == 1
        and memory.shape[1] == 8
        and rows == kv_count * NEW
        and rows % 16 == 0
        and width % TILE == 0
        and kv_count % groups == 0
        and w_gate.shape[1] % (kv_count // groups * TILE) == 0
        and NEW * 2 * all_heads == TILE
        and live_rows == groups * (GROUP - 1)
        and w_gate.shape[1] >= kv_count // groups * GROUP * TILE
    )


def layer(*arrays):
    if fits(arrays[0], arrays[2], arrays[8], arrays[15]):
        return fused_device(*arrays)
    return per_device(*arrays)


def solution(mesh):
    placed = (
        P(None, "kv"),
        P(),
        P("kv", "tp", None, None),
        P("kv"),
        P("kv", "tp"),
        P("kv", "tp"),
        P("kv", "tp"),
        P("kv", "tp"),
        P("kv", None),
        P("kv", None),
        P("tp"),
        P("tp"),
        P(),
        P("tp", "kv"),
        P("kv"),
        P("kv", "tp"),
        P("kv", "tp"),
        P("tp", "kv"),
    )
    return jax.shard_map(
        layer,
        mesh=mesh,
        in_specs=placed,
        out_specs=(P(None, "kv"), P("kv", "tp", None, None)),
        check_vma=False,
    )
```

```python
import jax
import jax.numpy as jnp
from jax import lax
from jax.experimental import pallas as pl
from jax.experimental.pallas import tpu as pltpu
from jax.sharding import PartitionSpec as P

D = 4096
DK = 128
DV = 128
NEW = 4


epsilon = 1e-06


def unit_rows(values):
    return values * lax.rsqrt(jnp.sum(values * values, axis=-1, keepdims=True) + epsilon)


def advance(memory, queries, key_rows, value_rows, decays, betas):
    outputs = []
    for step in range(queries.shape[1]):
        memory = jnp.exp(decays[:, step])[:, :, None, None] * memory
        predicted = jnp.einsum(
            "shde,shd->she", memory, key_rows[:, step], precision=lax.Precision.HIGHEST
        )
        correction = betas[:, step][:, :, None] * (value_rows[:, step] - predicted)
        memory = memory + key_rows[:, step][:, :, :, None] * correction[:, :, None, :]
        outputs.append(
            jnp.einsum("shde,shd->she", memory, queries[:, step], precision=lax.Precision.HIGHEST)
        )
    return (memory, jnp.stack(outputs, axis=1))


def per_device(
    tokens,
    lengths,
    memory,
    norm_gain,
    w_query,
    w_key,
    w_value,
    w_outgate,
    w_alpha,
    w_beta,
    decay_log,
    decay_bias,
    head_gain,
    w_output,
    mlp_gain,
    w_gate,
    w_up,
    w_down,
):
    total_rows = tokens.shape[0]
    kv_count = lax.axis_size("kv")
    kv_place = lax.axis_index("kv")
    tp_place = lax.axis_index("tp")
    own_rows = total_rows // kv_count
    seq_dev = memory.shape[0]
    heads_dev = memory.shape[1]
    token_f = tokens.astype(jnp.float32)
    squares = jnp.sum(token_f * token_f, axis=1)
    scaled = (token_f * norm_gain).astype(jnp.bfloat16)
    part_query = jnp.dot(scaled, w_query, preferred_element_type=jnp.float32)
    part_key = jnp.dot(scaled, w_key, preferred_element_type=jnp.float32)
    part_value = jnp.dot(scaled, w_value, preferred_element_type=jnp.float32)
    part_gate = jnp.dot(scaled, w_outgate, preferred_element_type=jnp.float32)
    part_alpha = jnp.dot(scaled, w_alpha, preferred_element_type=jnp.float32)
    part_beta = jnp.dot(scaled, w_beta, preferred_element_type=jnp.float32)
    all_squares = lax.psum(squares, "kv")
    sum_query, sum_key, sum_value, sum_gate, sum_alpha, sum_beta = (
        lax.psum_scatter(part_query, "kv", scatter_dimension=0, tiled=True),
        lax.psum_scatter(part_key, "kv", scatter_dimension=0, tiled=True),
        lax.psum_scatter(part_value, "kv", scatter_dimension=0, tiled=True),
        lax.psum_scatter(part_gate, "kv", scatter_dimension=0, tiled=True),
        lax.psum_scatter(part_alpha, "kv", scatter_dimension=0, tiled=True),
        lax.psum_scatter(part_beta, "kv", scatter_dimension=0, tiled=True),
    )
    own_squares = lax.dynamic_slice_in_dim(all_squares, kv_place * own_rows, own_rows)
    rstd = lax.rsqrt(own_squares / D + epsilon)[:, None]
    queries = (sum_query * rstd).astype(jnp.bfloat16)
    key_rows = (sum_key * rstd).astype(jnp.bfloat16)
    value_rows = (sum_value * rstd).astype(jnp.bfloat16)
    outgate = (sum_gate * rstd).astype(jnp.bfloat16)
    alphas = lax.dynamic_slice_in_dim(sum_alpha * rstd, tp_place * heads_dev, heads_dev, 1)
    beta_pre = lax.dynamic_slice_in_dim(sum_beta * rstd, tp_place * heads_dev, heads_dev, 1)
    own_lengths = lax.dynamic_slice_in_dim(lengths, kv_place * seq_dev, seq_dev)
    live = jnp.arange(NEW, dtype=jnp.int32)[None, :] < own_lengths[:, None]
    query_h = unit_rows(queries.astype(jnp.float32).reshape(seq_dev, NEW, heads_dev, DK)) * DK ** (
        -0.5
    )
    key_h = unit_rows(key_rows.astype(jnp.float32).reshape(seq_dev, NEW, heads_dev, DK))
    value_h = value_rows.astype(jnp.float32).reshape(seq_dev, NEW, heads_dev, DV)
    decays = -jnp.exp(decay_log) * jax.nn.softplus(alphas + decay_bias)
    decays = jnp.where(live[:, :, None], decays.reshape(seq_dev, NEW, heads_dev), 0.0)
    betas = jnp.where(
        live[:, :, None], jax.nn.sigmoid(beta_pre).reshape(seq_dev, NEW, heads_dev), 0.0
    )
    new_memory, attended = advance(memory, query_h, key_h, value_h, decays, betas)
    attended = attended * lax.rsqrt(jnp.mean(attended * attended, axis=-1, keepdims=True) + epsilon)
    gate_h = outgate.astype(jnp.float32).reshape(seq_dev, NEW, heads_dev, DV)
    mixed = (
        (attended * head_gain * jax.nn.silu(gate_h))
        .astype(jnp.bfloat16)
        .reshape(own_rows, heads_dev * DV)
    )
    attn_terms = jnp.dot(
        lax.all_gather(mixed, "kv", axis=0, tiled=True),
        w_output,
        preferred_element_type=jnp.float32,
    )
    attn_total = lax.psum(attn_terms, "tp")
    hidden = (token_f + attn_total).astype(jnp.bfloat16)
    hidden_f = hidden.astype(jnp.float32)
    hidden_squares = jnp.sum(hidden_f * hidden_f, axis=1)
    hscaled = (hidden_f * mlp_gain).astype(jnp.bfloat16)
    all_live = (jnp.arange(NEW, dtype=jnp.int32)[None, :] < lengths[:, None]).reshape(total_rows)
    part_gate_rows = jnp.dot(hscaled, w_gate, preferred_element_type=jnp.float32)
    part_up_rows = jnp.dot(hscaled, w_up, preferred_element_type=jnp.float32)
    gate_rows, up_rows, mlp_squares = lax.psum((part_gate_rows, part_up_rows, hidden_squares), "kv")
    rstd2 = lax.rsqrt(mlp_squares / D + epsilon)[:, None]
    active = (jax.nn.silu(gate_rows * rstd2) * (up_rows * rstd2)).astype(jnp.bfloat16)
    feed_terms = jnp.dot(active, w_down, preferred_element_type=jnp.float32)
    feed_total = lax.psum(feed_terms.astype(jnp.bfloat16), "tp").astype(jnp.float32)
    layer_out = jnp.where(all_live[:, None], hidden_f + feed_total, 0.0).astype(jnp.bfloat16)
    return (layer_out, new_memory)


F32 = jnp.float32
BF16 = jnp.bfloat16
HIGH = lax.Precision.HIGHEST
TILE = 128
GROUP = 8


def iota(shape, axis):
    return lax.broadcasted_iota(jnp.int32, shape, axis)


def dot(a, b, precision=None):
    return jnp.dot(a, b, preferred_element_type=F32, precision=precision)


def fused(
    lens_far,
    tokens_far,
    norm_far,
    decay_log_far,
    decay_bias_far,
    head_far,
    mlp_far,
    alpha_far,
    beta_far,
    memory,
    w_query,
    w_key,
    w_value,
    w_outgate,
    w_output,
    w_gate,
    w_up,
    w_down,
    out,
    v_mem,
    lens,
    tokens,
    norm_gain,
    decay_in,
    head_gain,
    mlp_gain,
    v_ab,
    v_proj,
    v_output,
    v_other,
    v_gu,
    v_down,
    proj_send,
    proj_recv,
    proj_part,
    proj_last,
    pf_recv,
    pf_part,
    pf_last,
    small_send,
    small_recv,
    small_part,
    small_last,
    rs_buf,
    xs_buf,
    kq_buf,
    m_split,
    r_buf,
    u_buf,
    a_buf,
    mix_buf,
    mix_all,
    tp_send,
    tp_recv,
    sq_send,
    sq_recv,
    gu_send,
    gu_recv,
    gu_part,
    gu_last,
    zf_recv,
    zf_part,
    zf_last,
    act_all,
    load_sem,
    send_sem,
    recv_sem,
    tp_sem,
):
    kv_count = mix_all.shape[0] // 2
    me = lax.axis_index("kv")
    tp = lax.axis_index("tp")
    rows, width = tokens.shape
    heads = v_mem.shape[0]
    wide = heads * DV
    compact = tp_send.shape[1]
    groups = compact // GROUP
    zones = kv_count // groups
    sent = gu_send.shape[2]
    chunk = sent + TILE
    held = GROUP - 1
    main = gu_recv.shape[2]
    wide_main = proj_recv.shape[2]
    total_width = width * kv_count
    all_heads = v_ab.shape[1]
    zone_me = me // groups
    group_me = lax.rem(me, groups)
    steps = [*range(1, zones), 0]
    side, odd = zone_me // 2, lax.rem(zone_me, 2)

    def zone_of(step):
        if zones != 4:
            return lax.rem(zone_me + step, zones)
        end = 1 - (side - odd) * (side - odd)
        far_end, near_end = (1 - side) * 3, side * 3
        far_mid, near_mid = 2 - side, 1 + side
        second = end * far_mid + (1 - end) * near_end
        third = end * near_mid + (1 - end) * far_mid
        return [zone_me, far_end, second, third][step]

    def peer(g):
        if groups != 4:
            return lax.rem(group_me + g, groups)
        row, col = group_me // 2, lax.rem(group_me, 2)
        return [
            group_me,
            (1 - row) * 2 + 1 - col,
            row * 2 + 1 - col,
            (1 - row) * 2 + col,
        ][g]

    barrier = pltpu.get_barrier_semaphore()

    def greet(**where):
        pl.semaphore_signal(
            barrier, inc=1, device_id=where, device_id_type=pl.DeviceIdType.MESH
        )

    for core in (tp, 1 - tp):
        for g in range(1, groups):
            greet(kv=zone_me * groups + peer(g), tp=core)
        for step in steps[:-1]:
            greet(kv=zone_of(step) * groups + group_me, tp=core)
    greet(tp=1 - tp)

    def load(src, dst, sem):
        return pltpu.make_async_copy(src, dst, load_sem.at[sem])

    part_wide = wide - wide_main
    pieces = wide // part_wide
    spans = [slice(c * part_wide, (c + 1) * part_wide) for c in range(pieces)][::-1]
    load(tokens_far, tokens, 0).start()
    load(norm_far, norm_gain, 1).start()
    load(alpha_far, v_ab.at[0], 2).start()
    load(beta_far, v_ab.at[1], 2).start()
    for c, span in enumerate(spans):
        for p, weight in enumerate((w_query, w_key, w_value, w_outgate)):
            load(weight.at[:, span], v_proj.at[p, :, span], 13 + c).start()
    load(lens_far, lens, 5).start()
    load(decay_log_far, decay_in.at[0], 6).start()
    load(decay_bias_far, decay_in.at[1], 6).start()
    load(head_far, head_gain, 7).start()
    load(mlp_far, mlp_gain, 8).start()

    def loaded(ref, sem):
        load(ref, ref, sem).wait()

    plane_sem, gu_sem, near_sem, far_sem = 0, zones, 3 * zones, 5 * zones
    proj_sem, mlp_sem, mix_sem, small_sem, few_sem, sq_sem = range(6 * zones, 6 * zones + 6)
    both_sem = 6 * zones + 6
    first_sem, then_sem = 6 * zones + 7, 6 * zones + 9
    early_sem, onward_sem = 6 * zones + 11, 6 * zones + 12
    mixed_sem, other_sem = 6 * zones + 13, 6 * zones + 14

    def remote(src, dst, sent, arrival, partner, core=None):
        return pltpu.make_async_remote_copy(
            src_ref=src,
            dst_ref=dst,
            send_sem=send_sem.at[sent],
            recv_sem=recv_sem.at[arrival],
            device_id={"kv": partner, "tp": tp if core is None else core},
            device_id_type=pl.DeviceIdType.MESH,
        )

    def arrived(ref, arrival):
        remote(ref, ref, 0, arrival, me).wait_recv()

    def left(ref, sent):
        remote(ref, ref, sent, 0, me).wait_send()

    def tp_swap(phase, value, meanwhile=None):
        tp_send[phase] = value
        swap = pltpu.make_async_remote_copy(
            src_ref=tp_send.at[phase],
            dst_ref=tp_recv.at[phase],
            send_sem=tp_sem.at[phase, 0],
            recv_sem=tp_sem.at[phase, 1],
            device_id={"tp": 1 - tp},
            device_id_type=pl.DeviceIdType.MESH,
        )
        swap.start()
        if meanwhile is not None:
            meanwhile()
        swap.wait()
        return value + tp_recv[phase]

    packed_rows = kv_count * 2 * NEW
    row = iota((packed_rows, rows), 0)
    spread = jnp.where(
        iota((packed_rows, rows), 1) == (row >> 3) * NEW + (row & 3), 1.0, 0.0
    ).astype(BF16)
    seq_row = iota((kv_count, rows), 0)
    seq_row = lax.rem(seq_row, zones) * groups + seq_row // zones
    lane = iota((kv_count, TILE), 1)
    place = iota((TILE, all_heads), 0) & (2 * all_heads - 1)
    head_of = iota((TILE, all_heads), 1)
    one_alpha = jnp.where(place == head_of, 1.0, 0.0).astype(BF16)
    one_beta = jnp.where(place == head_of + all_heads, 1.0, 0.0).astype(BF16)
    loaded(tokens, 0)
    loaded(norm_gain, 1)
    tok = tokens[...]
    scaled = (tok.astype(F32) * norm_gain[...]).astype(BF16)
    wide_scaled = dot(spread, scaled)
    part_of = iota((packed_rows, width), 0) & 7
    low = jnp.where(part_of < NEW, wide_scaled, 0.0).astype(BF16)
    high = jnp.where(part_of >= NEW, wide_scaled, 0.0).astype(BF16)

    def sum_plane(recv, sem, first, own):
        count = groups if own is None else groups - 1
        arrived(recv.at[pl.ds(first, count)], sem)
        added = (recv[first + group_me] if own is None else own).astype(F32)
        for g in range(1, groups):
            added = added + recv[first + peer(g)].astype(F32)
        return added

    def send_proj(zone, cols=slice(0, wide_main)):
        def send(slab, place, partner):
            remote(
                proj_send.at[slab, :, cols],
                proj_recv.at[place, :, cols],
                1,
                plane_sem + zone,
                partner,
                1 - tp,
            ).start()

        for g in range(1, groups):
            send(
                zone * groups + peer(g),
                zone * groups + group_me,
                zone_me * groups + peer(g),
            )
        send(zone * groups + group_me, zone * groups + group_me, me)

    for c, span in enumerate(spans):
        loaded(v_proj.at[:, :, span], 13 + c)
        parts = [
            dot(low, v_proj[p, :, span]) + dot(high, v_proj[p + 1, :, span]) for p in (0, 2)
        ]
        parts = [part.reshape(kv_count, 2 * NEW, part_wide) for part in parts]
        proj_send[:, :, span] = jnp.concatenate(parts, axis=1).astype(BF16)
        if c == 0:
            pl.semaphore_wait(barrier, 2 * (groups + zones - 2) + 1)
            for step in steps:
                zone = zone_of(step)
                remote(
                    proj_send.at[pl.ds(zone * groups, groups), :, span],
                    pf_recv.at[zone_me],
                    12,
                    early_sem,
                    zone * groups + group_me,
                    1 - tp,
                ).start()
        else:
            send_proj(zone_of(steps[0]), span)
    load(memory, v_mem, 9).start()
    load(w_output, v_output, 10).start()
    load(w_gate, v_gu.at[0], 11).start()
    load(w_up, v_gu.at[1], 11).start()
    load(w_down, v_down, 12).start()
    loaded(v_ab, 2)
    w_small = (dot(one_alpha, v_ab[0]) + dot(one_beta, v_ab[1])).astype(BF16)
    small = jnp.zeros((kv_count, TILE), F32)
    squares = jnp.zeros((kv_count, TILE), F32)
    for t in range(NEW):
        take = jnp.where(iota((kv_count, rows), 1) == seq_row * NEW + t, 1.0, 0.0).astype(BF16)
        took = lax.dot_general(
            dot(take, scaled).astype(BF16),
            w_small,
            (((1,), (1,)), ((), ())),
            preferred_element_type=F32,
        )
        small = jnp.where(lane // (2 * all_heads) == t, took, small)
        tok_t = dot(take, tok)
        squares = jnp.where(
            lane == t, jnp.sum(tok_t * tok_t, axis=1, keepdims=True), squares
        )
    small_send[:, :, 0, :] = small.reshape(groups, zones, TILE)
    small_send[:, :, 1, :] = squares.reshape(groups, zones, TILE)
    for g in range(1, groups):
        remote(
            small_send.at[peer(g)],
            small_recv.at[group_me],
            0,
            small_sem,
            zone_me * groups + peer(g),
        ).start()
    for step in steps[1:-1]:
        send_proj(zone_of(step))
    for g in range(1, groups):
        remote(
            proj_send.at[zone_me * groups + peer(g), :, :wide_main],
            proj_recv.at[me],
            1,
            plane_sem + zone_me,
            zone_me * groups + peer(g),
        ).start()

    loaded(lens, 5)
    loaded(decay_in, 6)
    loaded(head_gain, 7)
    loaded(mlp_gain, 8)
    slots_wide = kv_count * heads * NEW
    shape_a = (1, rows)
    shape_b = (1, slots_wide)
    shape_c = (rows, compact)
    length_a = jnp.zeros(shape_a, jnp.int32)
    start_a = jnp.zeros(shape_a, jnp.int32)
    length_b = jnp.zeros(shape_b, jnp.int32)
    start_b = jnp.zeros(shape_b, jnp.int32)
    length_c = jnp.zeros(shape_c, jnp.int32)
    start_c = jnp.zeros(shape_c, jnp.int32)
    seq_a = iota(shape_a, 1) >> 2
    seq_b = iota(shape_b, 1) >> 5
    seq_c = iota(shape_c, 0) >> 2
    begin = jnp.int32(0)
    for s in range(kv_count):
        length_a = jnp.where(seq_a == s, lens[s], length_a)
        start_a = jnp.where(seq_a == s, begin, start_a)
        length_b = jnp.where(seq_b == s, lens[s], length_b)
        start_b = jnp.where(seq_b == s, begin, start_b)
        length_c = jnp.where(seq_c == s, lens[s], length_c)
        start_c = jnp.where(seq_c == s, begin, start_c)
        begin = begin + lens[s]
    slot_a = iota(shape_a, 1) & 3

    def padded(rank):
        return sum(((rank >= g * held).astype(jnp.int32) for g in range(1, groups)), rank)

    rank_a = jnp.where(slot_a < length_a, padded(start_a + slot_a), -1)
    pack = jnp.where(rank_a == iota((compact, rows), 0), 1.0, 0.0).astype(BF16)
    slot_c = iota(shape_c, 0) & 3
    rank_c = jnp.where(slot_c < length_c, padded(start_c + slot_c), -1)
    unpack = jnp.where(rank_c == iota(shape_c, 1), 1.0, 0.0).astype(BF16)
    slot_b = iota(shape_b, 1) & 3
    head_b = (iota(shape_b, 1) >> 2) & (heads - 1)
    rank_b = jnp.where(slot_b < length_b, head_b * compact + padded(start_b + slot_b), -1)
    collect = jnp.where(rank_b == iota((heads * compact, slots_wide), 0), 1.0, 0.0).astype(BF16)
    tok_packed = dot(pack, tok)

    def proj_onward(zone):
        proj_part[zone] = sum_plane(proj_recv, plane_sem + zone, zone * groups, None).astype(BF16)
        remote(
            proj_part.at[zone],
            proj_last.at[zone_me],
            3,
            proj_sem,
            zone * groups + group_me,
            1 - tp,
        ).start()

    loaded(v_mem, 9)
    for h in range(heads):
        m_high = v_mem[h].astype(BF16)
        m_split[h, :, :DV] = m_high
        m_split[h, :, DV:] = (v_mem[h] - m_high.astype(F32)).astype(BF16)
    proj_onward(zone_of(steps[0]))
    arrived(small_recv.at[pl.ds(0, groups - 1)], small_sem)
    small = small_send[group_me]
    for g in range(1, groups):
        small = small + small_recv[peer(g)]
    small_part[...] = small
    for step in steps[:-1]:
        zone = zone_of(step)
        remote(
            small_part.at[zone], small_last.at[zone_me], 2, few_sem, zone * groups + group_me
        ).start()

    proj_onward(zone_of(steps[1]))
    arrived(pf_recv, early_sem)
    early = pf_recv[0].astype(F32)
    for zone in range(1, zones):
        early = early + pf_recv[zone].astype(F32)
    pf_part[...] = early.astype(BF16)
    for g in [*range(1, groups), 0]:
        remote(
            pf_part.at[peer(g)],
            pf_last.at[group_me],
            13,
            onward_sem,
            zone_me * groups + peer(g),
            1 - tp,
        ).start()
    for step in steps[2:-1]:
        proj_onward(zone_of(step))
    total = sum_plane(proj_recv, plane_sem + zone_me, zone_me * groups, proj_send[me, :, :wide_main])
    arrived(small_last.at[pl.ds(0, zones - 1)], few_sem)
    small = small_part[zone_me]
    for step in steps[:-1]:
        small = small + small_last[zone_of(step)]
    diagonal = iota((NEW, TILE), 0) == iota((NEW, TILE), 1)
    mean_sq = jnp.sum(jnp.where(diagonal, small[1:2, :], 0.0), axis=1, keepdims=True)
    rstd = lax.rsqrt(mean_sq / total_width + epsilon)
    rstd_wide = jnp.broadcast_to(rstd, (NEW, TILE))
    for p in range(4):
        rs_buf[p * NEW : (p + 1) * NEW, :] = rstd_wide
    eye = iota((heads, heads), 0) == iota((heads, heads), 1)
    rate = jnp.sum(jnp.where(eye, jnp.exp(decay_in[0]), 0.0), axis=1, keepdims=True)
    bias = jnp.sum(jnp.where(eye, decay_in[1], 0.0), axis=1, keepdims=True)
    pick = iota((heads, TILE), 1) - iota((heads, TILE), 0) - tp * heads
    own_length = jnp.full((heads, 1), lens[me], jnp.int32)
    decay, beta = [], []
    for t in range(NEW):
        line = small[0:1, :]
        first = 2 * all_heads * t
        scale_t = rstd[t : t + 1, :]
        alpha = jnp.sum(jnp.where(pick == first, line, 0.0), axis=1, keepdims=True) * scale_t
        write = (
            jnp.sum(jnp.where(pick == first + all_heads, line, 0.0), axis=1, keepdims=True)
            * scale_t
        )
        x = alpha + bias
        soft = jnp.maximum(x, 0.0) + jnp.log1p(jnp.exp(-jnp.abs(x)))
        live = own_length > t
        decay.append(jnp.exp(jnp.where(live, -rate * soft, 0.0)))
        beta.append(jnp.where(live, jax.nn.sigmoid(write), 0.0))
    arrived(proj_last.at[pl.ds(0, zones - 1)], proj_sem)
    for step in steps[:-1]:
        total = total + proj_last[zone_of(step)].astype(F32)
    arrived(pf_last, onward_sem)
    early = pf_last[0].astype(F32)
    for g in range(1, groups):
        early = early + pf_last[g].astype(F32)
    total = jnp.concatenate([total, early], axis=1)
    scale = rs_buf[...]
    for h in range(heads):
        piece = total[:, h * DV : (h + 1) * DV] * scale
        xs_buf[h * 16 : (h + 1) * 16, :] = piece.astype(BF16).astype(F32)

    def slot_rows(ref, index, stride):
        return ref[pl.ds(index, heads, stride=stride), :]

    query, key_rows, value, gate = (
        [slot_rows(xs_buf, p * NEW + t, 16) for t in range(NEW)] for p in range(4)
    )
    query = [unit_rows(x) * DK ** (-0.5) for x in query]
    key_rows = [unit_rows(x) for x in key_rows]
    for t in range(NEW):
        kq_buf[pl.ds(t, heads, stride=8), :] = key_rows[t]
        kq_buf[pl.ds(NEW + t, heads, stride=8), :] = query[t]
    for h in range(heads):
        kq = kq_buf[h * 8 : (h + 1) * 8, :]
        kq_high = kq.astype(BF16).astype(F32)
        both = dot(jnp.concatenate([kq_high, kq - kq_high], axis=0).astype(BF16), m_split[h])
        r_buf[h * 8 : (h + 1) * 8, :] = both[:8, :DV] + both[8:, :DV] + both[:8, DV:]
    seen_k = [slot_rows(r_buf, t, 8) for t in range(NEW)]
    seen_q = [slot_rows(r_buf, NEW + t, 8) for t in range(NEW)]

    def inner(a, b):
        return jnp.sum(a * b, axis=1, keepdims=True)

    corrections = []
    for t in range(NEW):
        for r in range(t, NEW):
            seen_k[r] = seen_k[r] * decay[t]
            seen_q[r] = seen_q[r] * decay[t]
        fix = beta[t] * (value[t] - seen_k[t])
        corrections.append(fix)
        for r in range(t, NEW):
            if r > t:
                seen_k[r] = seen_k[r] + inner(key_rows[t], key_rows[r]) * fix
            seen_q[r] = seen_q[r] + inner(key_rows[t], query[r]) * fix
    for t in range(NEW):
        o = seen_q[t]
        o = o * lax.rsqrt(jnp.mean(o * o, axis=1, keepdims=True) + epsilon)
        o = o * head_gain[...] * (gate[t] * jax.nn.sigmoid(gate[t]))
        mix_buf[pl.ds(t, heads, stride=NEW), :] = o
    own_mix = tp * kv_count + me
    mix_all[own_mix] = mix_buf[...].astype(BF16)

    def send_mix():
        for step in steps:
            for g in [*range(1, groups), 0]:
                if step or g:
                    to = zone_of(step) * groups + peer(g)
                    block = mix_all.at[own_mix]
                    remote(block, block, 4, mix_sem + tp * (mixed_sem - mix_sem), to, 1).start()

    send_mix()
    loaded(v_output, 10)

    @pl.when(tp == 0)
    def _():
        block = mix_all.at[own_mix]
        remote(block, block, 4, mix_sem, me, 1).start()
        remote(v_output, v_other, 14, other_sem, me, 1).start()

    u_buf[...] = jnp.zeros_like(u_buf)
    after = jnp.ones((heads, 1), F32)
    for t in range(NEW - 1, -1, -1):
        u_buf[pl.ds(t, heads, stride=8), :] = corrections[t] * after
        after = after * decay[t]
    a_buf[...] = jnp.broadcast_to(after, (heads, TILE))
    for h in range(heads):
        outer = lax.dot_general(
            kq_buf[h * 8 : (h + 1) * 8, :],
            u_buf[h * 8 : (h + 1) * 8, :],
            (((0,), (0,)), ((), ())),
            precision=HIGH,
            preferred_element_type=F32,
        )
        v_mem[h] = v_mem[h] * a_buf[h : h + 1, :] + outer
    loaded(v_gu, 11)
    loaded(v_down, 12)
    share = pltpu.make_async_remote_copy(
        src_ref=tp_recv.at[0],
        dst_ref=tp_recv.at[0],
        send_sem=tp_sem.at[0, 0],
        recv_sem=tp_sem.at[0, 1],
        device_id={"tp": 1 - tp},
        device_id_type=pl.DeviceIdType.MESH,
    )

    @pl.when(tp == 1)
    def _():
        def projected(core, weight):
            gathered = mix_all[pl.ds(core * kv_count, kv_count)].reshape(slots_wide, DV)
            packed = dot(collect, gathered).astype(BF16)
            packed = [packed[h * compact : (h + 1) * compact, :] for h in range(heads)]
            return dot(jnp.concatenate(packed, axis=1), weight[...])

        arrived(v_other, other_sem)
        arrived(mix_all.at[pl.ds(0, kv_count - 1)], mixed_sem)
        attended = projected(1, v_output)
        arrived(mix_all.at[pl.ds(0, kv_count)], mix_sem)
        tp_recv[0] = attended + projected(0, v_other)
        share.start()

    @pl.when(tp == 0)
    def _():
        share.wait_recv()

    attended = tp_recv[0]
    hidden = (tok_packed + attended).astype(BF16).astype(F32)

    hscaled = hidden * mlp_gain[...]
    blank = jnp.zeros((GROUP, width), F32)
    gate_rows = []
    for g in range(groups):
        gate_rows += [hscaled[g * GROUP : (g + 1) * GROUP, :], blank]
    gate_rows = jnp.concatenate(gate_rows, axis=0)
    up_rows = pltpu.roll(gate_rows, held, 0).astype(BF16)
    gate_rows = gate_rows.astype(BF16)
    spare = (iota((2 * compact, TILE), 0) & (2 * GROUP - 1)) >= 2 * held
    def product(zone, start, count):
        cols = pl.ds(pl.multiple_of(zone * chunk + start, TILE), count)
        return dot(gate_rows, v_gu[0, :, cols]) + dot(up_rows, v_gu[1, :, cols])

    def early_piece(turn):
        zone = zone_of(turn)
        piece = product(zone, main, sent - main).astype(BF16)
        here = pl.ds(zone * groups, groups)
        gu_send[here, :, main:] = piece.reshape(groups, 2 * GROUP, sent - main)
        rest = gu_send.at[here, :, main:]
        lands = zf_recv.at[tp * zones + zone_me]
        if turn:
            there = zone * groups + group_me
            remote(rest, lands, 10, first_sem + tp, there, 1).start()
        else:

            @pl.when(tp == 0)
            def _():
                remote(rest, lands, 10, first_sem, me, 1).start()

    for step in steps:
        zone = zone_of(step)
        term = product(zone, 0, main)
        last = product(zone, sent, TILE)
        tiles = [
            jnp.where(
                spare,
                pltpu.roll(last, 2 * (held - k), 0),
                term[:, k * TILE : (k + 1) * TILE],
            )
            for k in range(held)
        ]
        term = jnp.concatenate([*tiles, term[:, held * TILE : main]], axis=1)
        gu_send[pl.ds(zone * groups, groups), :, :main] = term.astype(BF16).reshape(
            groups, 2 * GROUP, main
        )
        arrival = gu_sem + tp * zones + zone
        for g in range(1, groups):
            remote(
                gu_send.at[zone * groups + peer(g), :, :main],
                gu_recv.at[tp * kv_count + zone * groups + group_me],
                6,
                arrival,
                zone_me * groups + peer(g),
                1,
            ).start()

        @pl.when(tp == 0)
        def _():
            slab = zone * groups + group_me
            remote(gu_send.at[slab, :, :main], gu_recv.at[slab], 6, arrival, me, 1).start()

        if step == steps[1]:
            for turn in steps:
                early_piece(turn)

        if step == steps[0]:

            @pl.when(tp == 1)
            def _():
                squares = jnp.sum(hidden * hidden, axis=1, keepdims=True)
                spot = (iota((compact, TILE), 0) & (GROUP - 1)) == iota((compact, TILE), 1)
                squares = jnp.sum(jnp.where(spot, squares, 0.0).reshape(groups, GROUP, TILE), axis=1)
                sq_send[...] = squares.reshape(groups, 1, TILE)
                sq_recv[me] = sq_send[group_me]

                @pl.loop(1, kv_count)
                def _(off):
                    to = lax.rem(me + off, kv_count)
                    remote(sq_send.at[lax.rem(to, groups)], sq_recv.at[me], 5, sq_sem, to).start()

    near_first = steps[::-1]

    @pl.when(tp == 1)
    def _():
        def plane_total(zone, core):
            slab = zone * groups
            own = gu_send[slab + group_me, :, :main] if core else None
            return sum_plane(gu_recv, gu_sem + core * zones + zone, core * kv_count + slab, own)

        def zones_total(core):
            arrived(zf_recv.at[pl.ds(core * zones, zones - core)], first_sem + core)
            if core:
                added = gu_send[pl.ds(zone_me * groups, groups), :, main:].astype(F32)
            else:
                added = zf_recv[zone_me].astype(F32)
            for step in steps[:-1]:
                added = added + zf_recv[core * zones + zone_of(step)].astype(F32)
            zf_part[pl.ds(core * groups, groups)] = added.astype(BF16)
            for g in range(1, groups):
                remote(
                    zf_part.at[core * groups + peer(g)],
                    zf_last.at[core * groups + group_me],
                    11,
                    then_sem + core,
                    zone_me * groups + peer(g),
                ).start()

        for step in steps[:-1]:
            zone = zone_of(step)
            for core in (0, 1):
                gu_part[core * zones + zone] = plane_total(zone, core).astype(BF16)
                remote(
                    gu_part.at[core * zones + zone],
                    gu_last.at[core * zones + zone_me],
                    7,
                    mlp_sem if core else both_sem,
                    zone * groups + group_me,
                ).start()
            if step == steps[1]:
                for core in (1, 0):
                    zones_total(core)
        arrived(sq_recv.at[pl.ds(0, kv_count - 1)], sq_sem)
        mean_sq = jnp.sum(sq_recv[...].reshape(kv_count, TILE), axis=0, keepdims=True)
        spot = iota((GROUP, TILE), 0) == iota((GROUP, TILE), 1)
        mean_sq = jnp.sum(jnp.where(spot, mean_sq, 0.0), axis=1, keepdims=True)
        rstd2 = lax.rsqrt(mean_sq / total_width + epsilon)

        def pass_on(zone, core, sent, arrival, partner, there):
            block = core * kv_count + zone * groups + group_me
            remote(act_all.at[block], act_all.at[block], sent, arrival, partner, there).start()

        def forward(zone, core):
            for g in range(1, groups):
                pass_on(zone, core, 9, far_sem + zone, zone_me * groups + peer(g), core)
            if core == 0:
                pass_on(zone, 0, 9, far_sem + zone, me, 0)

        for core in (0, 1):
            both = plane_total(zone_me, core)
            arrived(
                gu_last.at[pl.ds(core * zones, zones - 1)], mlp_sem if core else both_sem
            )
            for step in steps[:-1]:
                both = both + gu_last[core * zones + zone_of(step)].astype(F32)
            arrived(zf_last.at[pl.ds(core * groups, groups - 1)], then_sem + core)
            apart = zf_part[core * groups + group_me].astype(F32)
            for g in range(1, groups):
                apart = apart + zf_last[core * groups + peer(g)].astype(F32)
            both = jnp.concatenate([both, apart], axis=1)
            row = iota((2 * GROUP, TILE), 0)
            last = jnp.zeros((2 * GROUP, TILE), F32)
            for k in range(held):
                tile = both[:, k * TILE : (k + 1) * TILE]
                back = pltpu.roll(tile, 2 * GROUP - 2 * (held - k), 0)
                last = jnp.where(row >> 1 == k, back, last)
            both = jnp.concatenate([both, last], axis=1)
            gated = both[:GROUP] * rstd2
            lifted = pltpu.roll(both, 2 * GROUP - held, 0)[:GROUP] * rstd2
            active = gated * jax.nn.sigmoid(gated) * lifted
            row = iota((GROUP, TILE), 0)
            last = active[:, sent:]
            tiles = [
                jnp.where(
                    row == held,
                    last if k == held else pltpu.roll(last, held - k, 0),
                    active[:, k * TILE : (k + 1) * TILE],
                )
                for k in range(held)
            ]
            active = jnp.concatenate([*tiles, active[:, held * TILE : sent]], axis=1)
            act_all[core * kv_count + me] = active.astype(BF16)
            for step in steps[:-1]:
                there = zone_of(step) * groups + group_me
                pass_on(zone_me, core, 8, near_sem + core * zones + zone_me, there, 1)
            forward(zone_me, core)
        for step in near_first[1:]:
            zone = zone_of(step)
            for core in (0, 1):
                block = core * kv_count + zone * groups + group_me
                arrived(act_all.at[block], near_sem + core * zones + zone)
                forward(zone, core)

    feed = jnp.zeros((compact, width), F32)
    row_in = iota((compact, TILE), 0) & (GROUP - 1)
    for step in near_first:
        zone = zone_of(step)
        first = tp * kv_count + zone * groups

        @pl.when(tp == 0)
        def _():
            arrived(act_all.at[pl.ds(first, groups)], far_sem + zone)

        @pl.when(tp == 1)
        def _():
            arrived(act_all.at[pl.ds(first, groups - 1)], far_sem + zone)

        part = act_all[pl.ds(first, groups)].astype(F32).reshape(compact, sent)
        last = jnp.zeros((compact, TILE), F32)
        for k in range(held):
            tile = part[:, k * TILE : (k + 1) * TILE]
            last = jnp.where(row_in == k, pltpu.roll(tile, compact - (held - k), 0), last)
        part = jnp.concatenate([part, last], axis=1)
        cols = pl.ds(pl.multiple_of(zone * chunk, TILE), chunk)
        feed = feed + dot(part.astype(BF16), v_down[cols, :])

    def drain():
        left(small_send.at[pl.ds(0, groups - 1)], 0)
        left(proj_recv.at[pl.ds(0, kv_count - 1)], 1)
        left(pf_recv, 12)
        left(pf_last, 13)
        left(small_part.at[pl.ds(0, zones - 1)], 2)
        left(proj_part.at[pl.ds(0, zones - 1)], 3)

        @pl.when(tp == 0)
        def _():
            left(mix_all.at[pl.ds(0, kv_count)], 4)
            left(v_other, 14)
            left(gu_recv.at[pl.ds(0, kv_count)], 6)
            left(zf_recv.at[pl.ds(0, zones)], 10)

        @pl.when(tp == 1)
        def _():
            share.wait_send()
            left(mix_all.at[pl.ds(0, kv_count - 1)], 4)
            left(sq_recv.at[pl.ds(0, kv_count - 1)], 5)
            left(gu_recv.at[pl.ds(0, kv_count - zones)], 6)
            left(zf_recv.at[pl.ds(0, zones - 1)], 10)
            left(zf_last.at[pl.ds(0, 2 * (groups - 1))], 11)
            left(gu_part.at[pl.ds(0, 2 * (zones - 1))], 7)
            left(act_all.at[pl.ds(0, 2 * (zones - 1))], 8)
            left(act_all.at[pl.ds(0, zones * (2 * groups - 1))], 9)

    result = hidden + tp_swap(1, feed, drain)
    result = jnp.where((iota((compact, width), 0) & (GROUP - 1)) < held, result, 0.0)
    result = result.astype(BF16)
    out[...] = dot(unpack, result).astype(BF16)


def settle(out, state, out_far, state_far, sem):
    moves = [
        pltpu.make_async_copy(state, state_far, sem.at[0]),
        pltpu.make_async_copy(out, out_far, sem.at[1]),
    ]
    for move in moves:
        move.start()
    for move in moves:
        move.wait()


def fused_device(
    tokens,
    lengths,
    memory,
    norm_gain,
    w_query,
    w_key,
    w_value,
    w_outgate,
    w_alpha,
    w_beta,
    decay_log,
    decay_bias,
    head_gain,
    w_output,
    mlp_gain,
    w_gate,
    w_up,
    w_down,
):
    kv_count = lax.axis_size("kv")
    rows, width = tokens.shape
    heads = memory.shape[1]
    all_heads = w_alpha.shape[1]
    live_rows = (rows // NEW) * 7 // 4
    compact = -(-live_rows // 16) * 16
    groups = compact // GROUP
    zones = kv_count // groups
    sent = w_gate.shape[1] // zones - TILE
    main = sent - 2 * TILE
    wide = heads * DV
    early = 2 * TILE
    near = pl.BlockSpec(memory_space=pltpu.VMEM)
    far = pl.BlockSpec(memory_space=pltpu.HBM)
    out, state = pl.pallas_call(
        fused,
        out_shape=(
            jax.ShapeDtypeStruct((rows, width), BF16),
            jax.ShapeDtypeStruct(memory.shape[1:], F32),
        ),
        in_specs=[far] * 18,
        out_specs=(near, near),
        scratch_shapes=[
            pltpu.SMEM(lengths.shape, jnp.int32),
            pltpu.VMEM((rows, width), BF16),
            pltpu.VMEM((1, width), F32),
            pltpu.VMEM((2, 1, heads), F32),
            pltpu.VMEM((1, DV), F32),
            pltpu.VMEM((1, width), F32),
            pltpu.VMEM((2, all_heads, width), BF16),
            pltpu.VMEM((4, *w_query.shape), BF16),
            pltpu.VMEM(w_output.shape, BF16),
            pltpu.VMEM(w_output.shape, BF16),
            pltpu.VMEM((2, *w_gate.shape), BF16),
            pltpu.VMEM(w_down.shape, BF16),
            pltpu.VMEM((kv_count, 16, wide), BF16),
            pltpu.VMEM((kv_count, 16, wide - early), BF16),
            pltpu.VMEM((zones, 16, wide - early), BF16),
            pltpu.VMEM((zones, 16, wide - early), BF16),
            pltpu.VMEM((zones, groups, 16, early), BF16),
            pltpu.VMEM((groups, 16, early), BF16),
            pltpu.VMEM((groups, 16, early), BF16),
            pltpu.VMEM((groups, zones, 2, TILE), F32),
            pltpu.VMEM((groups, zones, 2, TILE), F32),
            pltpu.VMEM((zones, 2, TILE), F32),
            pltpu.VMEM((zones, 2, TILE), F32),
            pltpu.VMEM((16, TILE), F32),
            pltpu.VMEM((heads * 16, TILE), F32),
            pltpu.VMEM((heads * 8, TILE), F32),
            pltpu.VMEM((heads, DK, 2 * DV), BF16),
            pltpu.VMEM((heads * 8, TILE), F32),
            pltpu.VMEM((heads * 8, TILE), F32),
            pltpu.VMEM((heads, TILE), F32),
            pltpu.VMEM((heads * NEW, TILE), F32),
            pltpu.VMEM((2 * kv_count, heads * NEW, TILE), BF16),
            pltpu.VMEM((2, compact, width), F32),
            pltpu.VMEM((2, compact, width), F32),
            pltpu.VMEM((groups, 1, TILE), F32),
            pltpu.VMEM((kv_count, 1, TILE), F32),
            pltpu.VMEM((kv_count, 2 * GROUP, sent), BF16),
            pltpu.VMEM((2 * kv_count, 2 * GROUP, main), BF16),
            pltpu.VMEM((2 * zones, 2 * GROUP, main), BF16),
            pltpu.VMEM((2 * zones, 2 * GROUP, main), BF16),
            pltpu.VMEM((2 * zones, groups, 2 * GROUP, sent - main), BF16),
            pltpu.VMEM((2 * groups, 2 * GROUP, sent - main), BF16),
            pltpu.VMEM((2 * groups, 2 * GROUP, sent - main), BF16),
            pltpu.VMEM((2 * kv_count, GROUP, sent), BF16),
            pltpu.SemaphoreType.DMA((13 + wide // early,)),
            pltpu.SemaphoreType.DMA((15,)),
            pltpu.SemaphoreType.DMA((6 * zones + 15,)),
            pltpu.SemaphoreType.DMA((2, 2)),
        ],
        compiler_params=pltpu.CompilerParams(
            collective_id=0, has_side_effects=True, vmem_limit_bytes=48 * 1024 * 1024
        ),
    )(*[pltpu.with_memory_space_constraint(x, pltpu.HBM) for x in (
        lengths,
        tokens,
        norm_gain.reshape(1, -1),
        decay_log.reshape(1, -1),
        decay_bias.reshape(1, -1),
        head_gain.reshape(1, -1),
        mlp_gain.reshape(1, -1),
        w_alpha.T,
        w_beta.T,
        memory.reshape(memory.shape[1:]),
        w_query,
        w_key,
        w_value,
        w_outgate,
        w_output,
        w_gate,
        w_up,
        w_down,
    )])
    near = pl.BlockSpec(memory_space=pltpu.VMEM)
    out, state = pl.pallas_call(
        settle,
        out_shape=(
            jax.ShapeDtypeStruct(out.shape, out.dtype),
            jax.ShapeDtypeStruct(state.shape, state.dtype),
        ),
        in_specs=[near] * 2,
        out_specs=(far, far),
        scratch_shapes=[pltpu.SemaphoreType.DMA((2,))],
    )(*[pltpu.with_memory_space_constraint(x, pltpu.VMEM) for x in (out, state)])
    return out, state.reshape(memory.shape)


def fits(tokens, memory, w_alpha, w_gate):
    kv_count = lax.axis_size("kv")
    rows, width = tokens.shape
    live_rows = (rows // NEW) * 7 // 4
    groups = -(-live_rows // 16) * 16 // GROUP
    all_heads = w_alpha.shape[1]
    return (
        lax.axis_size("tp") == 2
        and memory.shape[0] == 1
        and memory.shape[1] == 8
        and rows == kv_count * NEW
        and rows % 16 == 0
        and width % TILE == 0
        and kv_count % groups == 0
        and w_gate.shape[1] % (kv_count // groups * TILE) == 0
        and NEW * 2 * all_heads == TILE
        and live_rows == groups * (GROUP - 1)
        and w_gate.shape[1] >= kv_count // groups * GROUP * TILE
    )


def layer(*arrays):
    if fits(arrays[0], arrays[2], arrays[8], arrays[15]):
        return fused_device(*arrays)
    return per_device(*arrays)


def solution(mesh):
    placed = (
        P(None, "kv"),
        P(),
        P("kv", "tp", None, None),
        P("kv"),
        P("kv", "tp"),
        P("kv", "tp"),
        P("kv", "tp"),
        P("kv", "tp"),
        P("kv", None),
        P("kv", None),
        P("tp"),
        P("tp"),
        P(),
        P("tp", "kv"),
        P("kv"),
        P("kv", "tp"),
        P("kv", "tp"),
        P("tp", "kv"),
    )
    return jax.shard_map(
        layer,
        mesh=mesh,
        in_specs=placed,
        out_specs=(P(None, "kv"), P("kv", "tp", None, None)),
        check_vma=False,
    )
```
